32 devices in a mesh: kv: 16 (over z, y, x), tp: 2 (over core).
Axes of the slice: x: 2, y: 2, z: 4, core: 2. Of those that a mesh axis runs over, the one named last changes fastest.
Arguments:
- tokens: bfloat16 [64, 4, 2048], P('kv', None, 'tp'), may hold values from -6 to 6
- input_gain: float32 [2048], replicated, may hold values from 0.1 to 1.9
- gate_weight: bfloat16 [2048, 4096], P('kv', 'tp'), may hold values from -0.125 to 0.125
- value_weight: bfloat16 [2048, 4096], P('kv', 'tp'), may hold values from -0.125 to 0.125
- write_weight: bfloat16 [2048, 1024], P('kv', 'tp'), may hold values from -0.125 to 0.125
- read_weight: bfloat16 [2048, 1024], P('kv', 'tp'), may hold values from -0.125 to 0.125
- step_weight: bfloat16 [2048, 64], replicated, may hold values from -0.125 to 0.125
- conv_value: float32 [4, 4096], P(None, 'tp'), may hold values from -3 to 3
- conv_write: float32 [4, 1024], P(None, 'tp'), may hold values from -3 to 3
- conv_read: float32 [4, 1024], P(None, 'tp'), may hold values from -3 to 3
- step_bias: float32 [64], P('tp'), may hold values from -4 to -1
- decay_log: float32 [64], P('tp'), may hold values from 0 to 2.8
- skip_gain: float32 [64], P('tp'), may hold values from 0.5 to 1.5
- output_gain: float32 [4096], P('tp'), may hold values from 0.1 to 1.9
- out_weight: bfloat16 [4096, 2048], P('tp', 'kv'), may hold values from -0.09375 to 0.09375
- base_state: float32 [64, 64, 64, 128], P('kv', 'tp'), may hold values from -2 to 2
- past_value: bfloat16 [64, 7, 4096], P('kv', None, 'tp'), may hold values from -6 to 6
- past_write: bfloat16 [64, 7, 1024], P('kv', None, 'tp'), may hold values from -6 to 6
- past_read: bfloat16 [64, 7, 1024], P('kv', None, 'tp'), may hold values from -6 to 6
- past_step: bfloat16 [64, 4, 64], P('kv', None, 'tp'), may hold values from -4 to 4
- accepted: int32 [64], P('kv'), may hold values from 1 to 4
Outputs:
- mixed: bfloat16 [64, 4, 2048], P('kv', None, 'tp')
- root_state: float32 [64, 64, 64, 128], P('kv', 'tp')
- next_value: bfloat16 [64, 7, 4096], P('kv', None, 'tp')
- next_write: bfloat16 [64, 7, 1024], P('kv', None, 'tp')
- next_read: bfloat16 [64, 7, 1024], P('kv', None, 'tp')
- next_step: bfloat16 [64, 4, 64], P('kv', None, 'tp')
The draws below stay inside these ranges and needn't reach their ends.
Inputs may be any that keep to these rules, and one draw needn't show every extreme that they name: Every entry of `accepted` is an integer from 1 to 4 (at least one of the last step's proposals is always accepted).
All inputs are finite; a program needn't handle non-finite values.
Results may differ from the reference program's by a relative error of at most 0.018.
Values may be sent and summed in bfloat16 or wider, within the bound.
A program may use at most 64 MiB of HBM per device.

```python
import jax
import jax.numpy as jnp
from jax import lax

WIDTH = 2048
INNER = 4096
HEADS = 64
HEAD_DIM = 64
GROUPS = 8
STATE_DIM = 128
CONV_W = 4
PROPOSALS = 4
SEQS = 64
PAST_ROWS = 7
N_TP = 2


def plant(entries, key, smallest, high):
    dims = entries.shape
    spot = [jax.random.randint(jax.random.fold_in(key, axis), (), 0, dims[axis]) for axis in range(len(dims))]
    entries = entries.at[tuple(spot)].set(smallest)
    longest = dims.index(max(dims))
    spot[longest] = (spot[longest] + 1) % dims[longest]
    return entries.at[tuple(spot)].set(high)


def levels(stream_key, shape, pieces, low, high):
    level = 1.0
    for dim, parts in pieces:
        draws = jax.random.uniform(jax.random.fold_in(jax.random.fold_in(stream_key, 6), dim), (parts,), jnp.float32, low / len(pieces), high / len(pieces))
        level = level * jnp.repeat(jnp.exp(draws), shape[dim] // parts).reshape((-1,) + (1,) * (len(shape) - 1 - dim))
    return level


def noise(key, extent, scale, most, shards=(), kind=jnp.bfloat16):
    loudness = levels(key, extent, shards, -0.22, 0.18) if shards else 1.0
    values = jax.random.normal(key, extent, jnp.float32) * scale * loudness
    return jnp.minimum(jnp.maximum(values, -most), most).astype(kind)


def setup_inputs(seed: int = 0) -> dict:
    key_of = jax.random.split(jax.random.key(seed), 22)
    tokens = noise(key_of[0], (SEQS, PROPOSALS, WIDTH), 1.0, 6.0, ((0, 16), (2, 2)))
    input_gain = jnp.clip(1.0 + 0.18 * jax.random.normal(key_of[1], (WIDTH,), jnp.float32), 0.1, 1.9)
    gate_weight = noise(key_of[2], (WIDTH, INNER), WIDTH ** -0.5, 0.125, ((0, 16), (1, 2)))
    value_weight = noise(key_of[3], (WIDTH, INNER), WIDTH ** -0.5, 0.125, ((0, 16), (1, 2)))
    write_weight = noise(key_of[4], (WIDTH, GROUPS * STATE_DIM), WIDTH ** -0.5, 0.125, ((0, 16), (1, 2)))
    read_weight = noise(key_of[5], (WIDTH, GROUPS * STATE_DIM), WIDTH ** -0.5, 0.125, ((0, 16), (1, 2)))
    step_weight = noise(key_of[6], (WIDTH, HEADS), WIDTH ** -0.5, 0.125)
    conv_value = noise(key_of[7], (CONV_W, INNER), 0.5, 3.0, ((1, 2),), jnp.float32)
    conv_write = noise(key_of[8], (CONV_W, GROUPS * STATE_DIM), 0.5, 3.0, ((1, 2),), jnp.float32)
    conv_read = noise(key_of[9], (CONV_W, GROUPS * STATE_DIM), 0.5, 3.0, ((1, 2),), jnp.float32)
    step_bias = jnp.clip(-4.0 + 3.0 * jax.random.uniform(key_of[10], (HEADS,), jnp.float32) ** levels(key_of[10], (HEADS,), ((0, 2),), -0.2, 0.2), -4.0, -1.0)
    decay_log = jnp.clip(2.8 * jax.random.uniform(key_of[11], (HEADS,), jnp.float32) ** levels(key_of[11], (HEADS,), ((0, 2),), -0.2, 0.2), 0.0, 2.8)
    skip_gain = jnp.clip(0.5 + 1.0 * jax.random.uniform(key_of[12], (HEADS,), jnp.float32) ** levels(key_of[12], (HEADS,), ((0, 2),), -0.2, 0.2), 0.5, 1.5)
    output_gain = jnp.clip(1.0 + 0.18 * jax.random.normal(key_of[13], (INNER,), jnp.float32), 0.1, 1.9)
    out_weight = noise(key_of[14], (INNER, WIDTH), INNER ** -0.5, 0.09375, ((0, 2), (1, 16)))
    base_state = noise(key_of[15], (SEQS, HEADS, HEAD_DIM, STATE_DIM), 0.3, 2.0, ((0, 16), (1, 2)), jnp.float32)
    past_value = noise(key_of[16], (SEQS, PAST_ROWS, INNER), 1.0, 6.0, ((0, 16), (2, 2)))
    past_write = noise(key_of[17], (SEQS, PAST_ROWS, GROUPS * STATE_DIM), 1.0, 6.0, ((0, 16), (2, 2)))
    past_read = noise(key_of[18], (SEQS, PAST_ROWS, GROUPS * STATE_DIM), 1.0, 6.0, ((0, 16), (2, 2)))
    past_step = noise(key_of[19], (SEQS, PROPOSALS, HEADS), 1.0, 4.0, ((0, 16), (2, 2)))
    accepted = plant(jax.random.randint(key_of[20], (SEQS,), 1, PROPOSALS + 1), jax.random.fold_in(key_of[20], 1), 1, PROPOSALS).astype(jnp.int32)
    return dict(tokens=tokens, input_gain=input_gain, gate_weight=gate_weight, value_weight=value_weight, write_weight=write_weight, read_weight=read_weight, step_weight=step_weight, conv_value=conv_value, conv_write=conv_write, conv_read=conv_read, step_bias=step_bias, decay_log=decay_log, skip_gain=skip_gain, output_gain=output_gain, out_weight=out_weight, base_state=base_state, past_value=past_value, past_write=past_write, past_read=past_read, past_step=past_step, accepted=accepted)


EPSILON = 1e-06

def causal_conv(rows, kernel):
    width = kernel.shape[0]
    count = rows.shape[0] - width + 1
    total = kernel[0] * rows[0:count]
    for offset in range(1, width):
        total = total + kernel[offset] * rows[offset:offset + count]
    return total

def advance(past_x, past_b, past_c, past_dt, taken, state_zero, value_now, write_now, read_now, gate_now, step_now, conv_value, conv_write, conv_read, step_bias, decay_log, skip_gain, output_gain):
    highest = lax.Precision.HIGHEST
    proposals = value_now.shape[0]
    head_count = step_bias.shape[0]
    group_count = write_now.shape[1] // STATE_DIM
    per_group = head_count // group_count
    head_width = value_now.shape[1] // head_count
    rate = jnp.exp(decay_log)
    taken = taken.astype(jnp.int32)
    prev_x = jax.nn.silu(causal_conv(past_x.astype(jnp.float32), conv_value)).reshape(proposals, head_count, head_width)
    prev_b = jax.nn.silu(causal_conv(past_b.astype(jnp.float32), conv_write)).reshape(proposals, group_count, STATE_DIM)
    prev_b = jnp.repeat(prev_b, per_group, axis=1)
    prev_dt = jax.nn.softplus(past_dt.astype(jnp.float32) + step_bias)
    live = (jnp.arange(proposals, dtype=jnp.int32) < taken)[:, None]
    prev_log = jnp.where(live, -rate * prev_dt, jnp.zeros_like(prev_dt))
    total_log = lax.optimization_barrier(jnp.sum(prev_log, axis=0))
    tail_log = total_log - jnp.cumsum(prev_log, axis=0)
    weight_now = jnp.where(live, jnp.exp(tail_log) * prev_dt, jnp.zeros_like(prev_dt))
    root = jnp.exp(total_log)[:, None, None] * state_zero + jnp.einsum('sh,shp,shn->hpn', weight_now, prev_x, prev_b, precision=highest)
    window_x = jnp.concatenate([lax.dynamic_slice_in_dim(past_x, taken, CONV_W - 1, 0), value_now], axis=0)
    window_b = jnp.concatenate([lax.dynamic_slice_in_dim(past_b, taken, CONV_W - 1, 0), write_now], axis=0)
    window_c = jnp.concatenate([lax.dynamic_slice_in_dim(past_c, taken, CONV_W - 1, 0), read_now], axis=0)
    cur_x = jax.nn.silu(causal_conv(window_x.astype(jnp.float32), conv_value)).reshape(proposals, head_count, head_width)
    cur_b = jax.nn.silu(causal_conv(window_b.astype(jnp.float32), conv_write)).reshape(proposals, group_count, STATE_DIM)
    cur_c = jax.nn.silu(causal_conv(window_c.astype(jnp.float32), conv_read)).reshape(proposals, group_count, STATE_DIM)
    cur_b = jnp.repeat(cur_b, per_group, axis=1)
    cur_c = jnp.repeat(cur_c, per_group, axis=1)
    cur_dt = jax.nn.softplus(step_now.astype(jnp.float32) + step_bias)
    logs = jnp.cumsum(-rate * cur_dt, axis=0)
    carried = jnp.einsum('thn,hpn->thp', cur_c, root, precision=highest) * jnp.exp(logs)[:, :, None]
    lower = (jnp.arange(proposals)[:, None] >= jnp.arange(proposals)[None, :])[:, :, None]
    diff = logs[:, None, :] - logs[None, :, :]
    decay = jnp.where(lower, jnp.exp(jnp.where(lower, diff, jnp.zeros_like(diff))), jnp.zeros_like(diff))
    scores = jnp.einsum('thn,shn->tsh', cur_c, cur_b, precision=highest) * decay * cur_dt[None, :, :]
    inner = jnp.einsum('tsh,shp->thp', scores, cur_x, precision=highest)
    mixed = carried + inner + skip_gain[None, :, None] * cur_x
    gated = mixed.reshape(proposals, -1) * jax.nn.silu(gate_now.astype(jnp.float32))
    grouped = gated.reshape(proposals, group_count, -1)
    grouped = grouped * lax.rsqrt(lax.optimization_barrier(jnp.mean(grouped * grouped, axis=-1, keepdims=True)) + EPSILON)
    result = (grouped.reshape(proposals, -1) * output_gain).astype(jnp.bfloat16)
    return (result, root, window_x, window_b, window_c)

def reference(tokens, input_gain, gate_weight, value_weight, write_weight, read_weight, step_weight, conv_value, conv_write, conv_read, step_bias, decay_log, skip_gain, output_gain, out_weight, base_state, past_value, past_write, past_read, past_step, accepted):
    seq_count, proposals, width = tokens.shape
    rows = tokens.astype(jnp.float32)
    normed = (rows * lax.rsqrt(lax.optimization_barrier(jnp.mean(rows * rows, axis=-1, keepdims=True)) + EPSILON) * input_gain).astype(jnp.bfloat16)
    flat = normed.reshape(seq_count * proposals, width)

    def project(weight):
        product = jnp.dot(flat, weight, preferred_element_type=jnp.float32).astype(jnp.bfloat16)
        return product.reshape(seq_count, proposals, weight.shape[1])
    gate_now = project(gate_weight)
    value_now = project(value_weight)
    write_now = project(write_weight)
    read_now = project(read_weight)
    step_now = project(step_weight)

    def one_sequence(items):
        return advance(*items, conv_value, conv_write, conv_read, step_bias, decay_log, skip_gain, output_gain)
    normal_out, root_state, next_value, next_write, next_read = lax.map(one_sequence, (past_value, past_write, past_read, past_step, accepted, base_state, value_now, write_now, read_now, gate_now, step_now))
    flat_y = normal_out.reshape(seq_count * proposals, -1)
    block = flat_y.shape[1] // N_TP
    total = jnp.zeros((seq_count * proposals, width), jnp.float32)
    for portion in range(N_TP):
        partial_sum = jnp.dot(flat_y[:, portion * block:(portion + 1) * block], out_weight[portion * block:(portion + 1) * block], preferred_element_type=jnp.float32)
        total = total + lax.optimization_barrier(partial_sum.astype(jnp.bfloat16)).astype(jnp.float32)
    mixed = total.astype(jnp.bfloat16).reshape(seq_count, proposals, width)
    return (mixed, root_state, next_value, next_write, next_read, step_now)
```

```python
import functools
from typing import NamedTuple

import jax
import jax.numpy as jnp
from jax import lax
from jax.experimental import pallas as pl
from jax.experimental.pallas import tpu as pltpu
from jax.sharding import PartitionSpec as P

STATE_DIM = 128
LANES = 128
EPSILON = 1e-06
MESH = pl.DeviceIdType.MESH
F32 = jnp.float32
BF16 = jnp.bfloat16


class Dims(NamedTuple):
    far: int
    near: int
    n_tp: int
    seqs: int
    props: int
    taps: int
    width: int
    feats: int
    depth: int
    groups: int
    gw: int
    heads: int
    out_cols: int

    @property
    def rows(self):
        return self.seqs * self.props

    @property
    def n_kv(self):
        return self.far * self.near

    @property
    def block(self):
        return self.near * self.depth

    @property
    def part(self):
        return self.gw // self.near

    @property
    def every(self):
        return self.near // 2

    def thin(self, g):
        return g % self.every == 0

    def cols(self, g):
        return 2 * self.part + (STATE_DIM if self.thin(g) else 0)


def near_size(n_kv, gw):
    return max(
        d
        for d in range(2, n_kv + 1, 2)
        if n_kv % d == 0 and d * d <= n_kv and gw % (LANES * d) == 0
    )


def remote(src, dst, send, recv, kv, tp):
    return pltpu.make_async_remote_copy(
        src_ref=src,
        dst_ref=dst,
        send_sem=send,
        recv_sem=recv,
        device_id={"kv": kv, "tp": tp},
        device_id_type=MESH,
    )


def silu(v):
    return v / (1.0 + jnp.exp(-v))


def softplus(v):
    return jnp.maximum(v, 0.0) + jnp.log1p(jnp.exp(-jnp.abs(v)))


def conv(rows, taps, count):
    out = []
    for t in range(count):
        total = taps[0] * rows[t]
        for k in range(1, len(taps)):
            total = total + taps[k] * rows[t + k]
        out.append(total)
    return out


NT = (((1,), (1,)), ((), ()))


def mixer_kernel(d, *refs):
    (
        tok, gain, gate_w, value_w, write_w, read_w, step_w, conv_v, conv_b, conv_c, head_p,
        wout_h, base_h, past_v, past_b, past_c, past_s, taken_ref,
    ) = refs[:18]
    mixed, root_h, next_v, next_b, next_c, next_s = refs[18:24]
    rest = list(refs[24:])
    G = d.groups
    stage, wbuf, zmine, zin, red, back, rootb, ys = (rest[i * G : (i + 1) * G] for i in range(8))
    (
        xq, xs, pt_mine, pt_in, base_v, wout, acc, mine, parts,
        ssem, w_sem, xz_sem, xp_sem, pt_sem, z_sem, b_sem, y_sem, m_sem, l_sem,
    ) = rest[8 * G :]
    far, near, n_tp, rows, S, N = d.far, d.near, d.n_tp, d.rows, d.seqs, STATE_DIM
    n_kv, part, gw, props = d.n_kv, d.part, d.gw, d.props
    me, tp = lax.axis_index("kv"), lax.axis_index("tp")
    h, l = lax.div(me, near), lax.rem(me, near)

    total = n_kv * n_tp
    flat = me * n_tp + tp
    barrier = pltpu.get_barrier_semaphore()

    def greet(step, carry):
        other = lax.rem(flat + step, total)
        pl.semaphore_signal(
            barrier,
            inc=1,
            device_id={"kv": lax.div(other, n_tp), "tp": lax.rem(other, n_tp)},
            device_id_type=MESH,
        )
        return carry

    lax.fori_loop(1, total, greet, 0)

    used = []

    def local(src, dst):
        copy = pltpu.make_async_copy(src, dst, l_sem.at[len(used)])
        copy.start()
        used.append(copy)
        return copy

    units = 2 * G
    staging = []
    for g in range(G):
        copies = []
        for k in range(near):
            lo = g * gw + k * part
            copies.append(local(gate_w.at[:, lo : lo + part], stage[g].at[k, :, 0:part]))
            copies.append(local(value_w.at[:, lo : lo + part], stage[g].at[k, :, part : 2 * part]))
            if d.thin(g):
                u = (g // d.every * near + k) % units
                source = (write_w, read_w)[u % 2]
                copies.append(
                    local(
                        source.at[:, u // 2 * N : (u // 2 + 1) * N],
                        stage[g].at[k, :, 2 * part : 2 * part + N],
                    )
                )
        staging.append(copies)
    loading = [
        local(base_h.at[:, g * gw : (g + 1) * gw], base_v.at[:, g * gw : (g + 1) * gw])
        for g in range(G)
    ]
    wout_load = local(wout_h, wout)

    sends = []

    def send(src, dst, recv, kv, t, cond=None):
        copy = remote(src, dst, ssem.at[len(sends)], recv, kv, t)
        sends.append((copy, cond))
        if cond is None:
            copy.start()
        else:
            pl.when(cond)(copy.start)

    def arrive(dst, recv, cond=None):
        copy = remote(dst, dst, ssem.at[0], recv, me, tp)
        if cond is None:
            copy.wait_recv()
        else:
            pl.when(cond)(copy.wait_recv)

    nb = d.feats // d.block
    own = pl.multiple_of(tp * d.feats, d.feats)
    raw = tok[...].astype(F32)
    square = jnp.sum(raw * raw, axis=-1, keepdims=True)
    scaled = (raw * gain[:, pl.ds(own, d.feats)]).astype(BF16)
    for q in range(nb):
        xq[q] = scaled[:, q * d.block : (q + 1) * d.block]
    hpad = pt_mine.shape[2] - LANES
    for t in range(n_tp):
        term = lax.dot_general(
            scaled, step_w[t * d.heads : (t + 1) * d.heads, pl.ds(own, d.feats)], NT,
            preferred_element_type=F32,
        )
        pt_mine[t, :, 0 : d.heads] = term
        pt_mine[t, :, hpad : hpad + LANES] = jnp.broadcast_to(square, (rows, LANES))
    pt_in[tp] = pt_mine[tp]

    pl.semaphore_wait(barrier, total - 1)

    home = lax.div(h, nb)
    for q in range(nb):
        plane = tp * nb + q
        for t in range(n_tp):
            away = jnp.logical_or(plane != h, tp != t)
            send(xq.at[q], xs.at[l, h], xz_sem.at[h], plane * near + l, t, away)

    @pl.when(home == tp)
    def _():
        xs[l, h] = xq[lax.rem(h, nb)]

    for step in range(1, n_tp):
        t = lax.rem(tp + step, n_tp)
        send(pt_mine.at[t], pt_in.at[tp], pt_sem.at[tp], me, t)

    def send_weights(g):
        for copy in staging[g]:
            copy.wait()
        for step in range(1, near):
            k = lax.rem(l + step, near)
            send(stage[g].at[k], wbuf[g].at[l], w_sem.at[g, l], h * near + k, tp)

    send_weights(0)

    taken = taken_ref[...]
    row_seq = lax.rem(lax.broadcasted_iota(jnp.int32, (rows, N), 0), S)

    def spread(g):
        r = lax.broadcasted_iota(jnp.int32, (d.heads, gw), 0)
        c = lax.broadcasted_iota(jnp.int32, (d.heads, gw), 1)
        hw = gw * G // d.heads
        lo = r * hw - g * gw
        return jnp.where(jnp.logical_and(c >= lo, c < lo + hw), 1.0, 0.0).astype(BF16)

    def span(g, w):
        return slice(g * w, (g + 1) * w)

    def taps(ref, cols):
        return [ref[k : k + 1, cols] for k in range(d.taps)]

    def param(k, g):
        return head_p[k : k + 1, span(g, gw)]

    def pieces(v):
        return [v[t * S : (t + 1) * S] for t in range(props)]

    def old(ref, cols):
        return [ref[i, :, cols].astype(F32) for i in range(ref.shape[0])]

    def root(g):
        loading[g].wait()
        cv, cn = span(g, gw), span(g, N)
        px = [silu(v) for v in conv(old(past_v, cv), taps(conv_v, cv), props)]
        pb = [silu(v) for v in conv(old(past_b, cn), taps(conv_b, cn), props)]
        pd = softplus(
            jnp.dot(past_s[...], spread(g), preferred_element_type=F32) + param(0, g)
        )
        rate = jnp.exp(param(1, g))
        pd = pieces(pd)
        log = [jnp.where(taken > t, -rate * pd[t], 0.0) for t in range(props)]
        tail = jnp.zeros_like(log[0])
        weighted = [None] * props
        for t in reversed(range(props)):
            weighted[t] = jnp.where(taken > t, jnp.exp(tail) * pd[t], 0.0) * px[t]
            tail = tail + log[t]
        left = jnp.transpose(jnp.concatenate(weighted, axis=0)).astype(BF16)
        decay = jnp.exp(tail)
        fill = [decay] * max(1, 8 // S)
        decay = jnp.transpose(jnp.concatenate(fill, axis=0))
        right = jnp.concatenate(pb, axis=0)
        for s in range(S):
            outer = jnp.dot(
                left,
                jnp.where(row_seq == s, right, 0.0).astype(BF16),
                preferred_element_type=F32,
            )
            new = decay[:, s : s + 1] * base_v[s, cv, :] + outer
            base_v[s, cv, :] = new
            rootb[g][:, span(s, N)] = new.astype(BF16)
        return local(base_v.at[:, cv], root_h.at[:, cv])

    stores = [root(0)]

    for k in range(far):
        arrive(
            xs.at[l, k], xz_sem.at[k], jnp.logical_or(h != k, home != tp)
        )
    for step in range(1, near):
        send(xs.at[l], xs.at[l], xp_sem.at[l], h * near + lax.rem(l + step, near), tp)
    for g in range(1, G):
        send_weights(g)

    for step in range(1, n_tp):
        t = lax.rem(tp + n_tp - step, n_tp)
        arrive(pt_in.at[t], pt_sem.at[t])
    joined = pt_in[0]
    for t in range(1, n_tp):
        joined = joined + pt_in[t]
    scale = lax.rsqrt(joined[:, hpad : hpad + LANES] * (1.0 / d.width) + EPSILON)
    step_now = (joined[:, 0 : d.heads] * scale[:, 0 : d.heads]).astype(BF16)
    next_s[...] = step_now

    for step in range(1, near):
        k = lax.rem(l + near - step, near)
        arrive(xs.at[k], xp_sem.at[k])

    def project(g):
        wbuf[g][l] = stage[g][l]
        for step in range(1, near):
            k = lax.rem(l + near - step, near)
            arrive(wbuf[g].at[k], w_sem.at[g, k])
        cols = d.cols(g)
        product = jnp.dot(
            xs[...].reshape(n_kv * rows, d.block),
            wbuf[g][...].reshape(d.block, cols),
            preferred_element_type=F32,
        ).astype(BF16)
        for k in range(near):
            for z in range(far):
                at = (k * far + z) * rows
                zmine[g][z, k] = product[at : at + rows]
        for step in range(1, far):
            z = lax.rem(h + step, far)
            send(zmine[g].at[z], zin[g].at[h], z_sem.at[g, h], z * near + l, tp)

    def collect(g):
        value = zmine[g][h].astype(F32)
        for step in range(1, far):
            z = lax.rem(h + far - step, far)
            arrive(zin[g].at[z], z_sem.at[g, z])
            value = value + zin[g][z].astype(F32)
        red[g][...] = value.astype(BF16)
        back[g][l] = red[g][l]
        for step in range(1, near):
            k = lax.rem(l + step, near)
            send(red[g].at[k], back[g].at[l], b_sem.at[g, l], h * near + k, tp)

    def rounded(piece):
        return (piece.astype(F32) * scale).astype(BF16).astype(F32)

    def advance(g):
        for step in range(1, near):
            k = lax.rem(l + near - step, near)
            arrive(back[g].at[k], b_sem.at[g, k])
        cv, cn = span(g, gw), span(g, N)
        gate = jnp.concatenate([rounded(back[g][k, :, 0:part]) for k in range(near)], axis=1)
        value = jnp.concatenate(
            [rounded(back[g][k, :, part : 2 * part]) for k in range(near)], axis=1
        )

        def unit(u):
            j, k = u // near, u % near
            return rounded(back[j * d.every][k, :, 2 * part : 2 * part + N])

        def window(past, now, out, cols):
            before = old(past, cols)
            rows_now = []
            for i in range(d.taps - 1):
                row = before[i + 1]
                for a in range(2, props + 1):
                    row = jnp.where(taken == a, before[i + a], row)
                rows_now.append(row)
            rows_now = rows_now + pieces(now)
            for i, row in enumerate(rows_now):
                out[i, :, cols] = row.astype(BF16)
            return rows_now

        win_v = window(past_v, value, next_v, cv)
        win_b = window(past_b, unit(2 * g), next_b, cn)
        win_c = window(past_c, unit(2 * g + 1), next_c, cn)
        x = [silu(v) for v in conv(win_v, taps(conv_v, cv), props)]
        b = [silu(v) for v in conv(win_b, taps(conv_b, cn), props)]
        c = [silu(v) for v in conv(win_c, taps(conv_c, cn), props)]
        whole = jnp.concatenate(c, axis=0)
        masked = jnp.concatenate(
            [jnp.where(row_seq == s, whole, 0.0) for s in range(S)], axis=1
        ).astype(BF16)
        carried = pieces(
            lax.dot_general(masked, rootb[g][...], NT, preferred_element_type=F32)
        )
        dt = pieces(
            softplus(jnp.dot(step_now, spread(g), preferred_element_type=F32) + param(0, g))
        )
        rate = jnp.exp(param(1, g))
        logs = []
        for t in range(props):
            log = -rate * dt[t]
            logs.append(log if t == 0 else logs[-1] + log)
        y = []
        for t in range(props):
            row = jnp.exp(logs[t]) * carried[t] + param(2, g) * x[t]
            for s in range(t + 1):
                score = jnp.sum(c[t] * b[s], axis=-1, keepdims=True)
                weight = dt[s] if s == t else jnp.exp(logs[t] - logs[s]) * dt[s]
                row = row + (score * weight) * x[s]
            y.append(row)
        gated = jnp.concatenate(y, axis=0) * silu(gate)
        mean = jnp.sum(gated * gated, axis=-1, keepdims=True) * (1.0 / gw)
        ys[g][me] = (gated * lax.rsqrt(mean + EPSILON) * param(3, g)).astype(BF16)
        for step in range(1, far):
            z = lax.rem(h + step, far)
            send(ys[g].at[me], ys[g].at[me], y_sem.at[g, me], z * near + l, tp)
        for step in range(1, near):
            k = lax.rem(l + step, near)
            send(ys[g].at[me], ys[g].at[me], y_sem.at[g, me], h * near + k, tp)

    def forward(g):
        for step in range(1, far):
            block = lax.rem(h + far - step, far) * near + l
            arrive(ys[g].at[block], y_sem.at[g, block])
            for side in range(1, near):
                k = lax.rem(l + side, near)
                send(ys[g].at[block], ys[g].at[block], y_sem.at[g, block], h * near + k, tp)

    def output(g):
        for side in range(1, near):
            k = lax.rem(l + near - side, near)
            for step in range(far):
                block = lax.rem(h + far - step, far) * near + k
                arrive(ys[g].at[block], y_sem.at[g, block])
        if g == 0:
            wout_load.wait()
        term = jnp.dot(
            ys[g][...].reshape(n_kv * rows, gw), wout[span(g, gw), :], preferred_element_type=F32
        )
        if g == 0:
            acc[...] = term
        else:
            acc[...] += term

    lag = {"root": -1, "collect": 2, "advance": 3, "forward": 4, "output": 5}
    for i in range(G + max(lag.values())):
        if i < G:
            project(i)
        if 0 < i + 1 < G:
            stores.append(root(i + 1))
        for name, stage_fn in (
            ("collect", collect), ("advance", advance), ("forward", forward), ("output", output),
        ):
            g = i - lag[name]
            if 0 <= g < G:
                stage_fn(g)

    cols = d.out_cols
    mine[...] = acc[...].astype(BF16).reshape(n_kv, rows, cols)
    per = n_kv // n_tp
    side, place = lax.div(me, per), lax.rem(me, per)
    for step in range(n_kv):
        k = lax.rem(me + step, n_kv)
        send(
            mine.at[k], parts.at[tp, place], m_sem.at[tp, place], k, side,
            (side != tp) if step == 0 else None,
        )

    @pl.when(side == tp)
    def _():
        parts[tp, place] = mine[me]

    for t in range(n_tp):
        for k in range(per):
            arrive(
                parts.at[t, k], m_sem.at[t, k], jnp.logical_or(t != tp, tp * per + k != me)
            )
    for k in range(per):
        value = parts[0, k].astype(F32)
        for t in range(1, n_tp):
            value = value + parts[t, k].astype(F32)
        mixed[:, span(k, cols)] = value.astype(BF16)
    for copy, cond in sends:
        if cond is None:
            copy.wait_send()
        else:
            pl.when(cond)(copy.wait_send)
    for copy in stores:
        copy.wait()


def mixer(d, args):
    G, near, far, rows, n_kv = d.groups, d.near, d.far, d.rows, d.n_kv
    dma = pltpu.SemaphoreType.DMA
    vmem, any_ = pl.BlockSpec(memory_space=pltpu.VMEM), pl.BlockSpec(memory_space=pl.ANY)

    def each(shape):
        return [pltpu.VMEM(shape(g), BF16) for g in range(G)]

    scratch = (
        each(lambda g: (near, d.depth, d.cols(g)))
        + each(lambda g: (near, d.depth, d.cols(g)))
        + each(lambda g: (far, near, rows, d.cols(g)))
        + each(lambda g: (far, near, rows, d.cols(g)))
        + each(lambda g: (near, rows, d.cols(g)))
        + each(lambda g: (near, rows, d.cols(g)))
        + each(lambda g: (d.gw, d.seqs * STATE_DIM))
        + each(lambda g: (n_kv, rows, d.gw))
    )
    nb = d.feats // d.block
    hpad = -(-d.heads // LANES) * LANES
    per = n_kv // d.n_tp
    n_send = (
        nb * d.n_tp + d.n_tp - 1 + near - 1
        + G * (2 * (near - 1) + far - 1)
        + G * (far - 1 + (near - 1) * far)
        + n_kv
    )
    n_local = sum(near * (3 if d.thin(g) else 2) for g in range(G)) + 2 * G + 1
    scratch = scratch + [
        pltpu.VMEM((nb, rows, d.block), BF16),
        pltpu.VMEM((near, far, rows, d.block), BF16),
        pltpu.VMEM((d.n_tp, rows, hpad + LANES), F32),
        pltpu.VMEM((d.n_tp, rows, hpad + LANES), F32),
        pltpu.VMEM((d.seqs, G * d.gw, STATE_DIM), F32),
        pltpu.VMEM((G * d.gw, d.out_cols), BF16),
        pltpu.VMEM((n_kv * rows, d.out_cols), F32),
        pltpu.VMEM((n_kv, rows, d.out_cols), BF16),
        pltpu.VMEM((d.n_tp, per, rows, d.out_cols), BF16),
        dma((n_send,)), dma((G, near)), dma((far,)), dma((near,)), dma((d.n_tp,)),
        dma((G, far)), dma((G, near)), dma((G, n_kv)), dma((d.n_tp, per)), dma((n_local,)),
    ]
    specs = [vmem] * len(args)
    for i in (2, 3, 4, 5, 11, 12):
        specs[i] = any_
    past_rows = args[13].shape[0]
    out_shape = [
        jax.ShapeDtypeStruct((rows, d.feats), BF16),
        jax.ShapeDtypeStruct((d.seqs, G * d.gw, STATE_DIM), F32),
        jax.ShapeDtypeStruct((past_rows, d.seqs, G * d.gw), BF16),
        jax.ShapeDtypeStruct((past_rows, d.seqs, G * STATE_DIM), BF16),
        jax.ShapeDtypeStruct((past_rows, d.seqs, G * STATE_DIM), BF16),
        jax.ShapeDtypeStruct((rows, d.heads), BF16),
    ]
    return pl.pallas_call(
        functools.partial(mixer_kernel, d),
        out_shape=out_shape,
        in_specs=specs,
        out_specs=[vmem, any_, vmem, vmem, vmem, vmem],
        scratch_shapes=scratch,
        compiler_params=pltpu.CompilerParams(collective_id=0, has_side_effects=True),
        name="mixer",
    )(*args)


def on_device(
    tokens, input_gain, gate_weight, value_weight, write_weight, read_weight, step_weight,
    conv_value, conv_write, conv_read, step_bias, decay_log, skip_gain, output_gain, out_weight,
    base_state, past_value, past_write, past_read, past_step, accepted,
):
    seqs, props, feats = tokens.shape
    n_kv, n_tp = lax.axis_size("kv"), lax.axis_size("tp")
    depth, inner = gate_weight.shape
    groups = write_weight.shape[1] // STATE_DIM
    heads = step_bias.shape[0]
    gw = inner // groups
    near = near_size(n_kv, gw)
    d = Dims(
        far=n_kv // near, near=near, n_tp=n_tp, seqs=seqs, props=props,
        taps=conv_value.shape[0], width=feats * n_tp, feats=feats, depth=depth, groups=groups,
        gw=gw, heads=heads, out_cols=out_weight.shape[1],
    )

    def major(item):
        return item.transpose(1, 0, 2)

    def per_head(item):
        return jnp.repeat(item, inner // heads)

    head_p = jnp.stack([per_head(step_bias), per_head(decay_log), per_head(skip_gain), output_gain])
    mixed, root, next_v, next_b, next_c, next_s = mixer(
        d,
        (
            major(tokens).reshape(d.rows, feats),
            input_gain.reshape(1, d.width),
            gate_weight, value_weight, write_weight, read_weight,
            step_weight.T,
            conv_value, conv_write, conv_read,
            head_p,
            out_weight,
            base_state.reshape(seqs, inner, STATE_DIM),
            major(past_value), major(past_write), major(past_read),
            major(past_step).reshape(d.rows, heads),
            accepted.reshape(seqs, 1),
        ),
    )
    return (
        major(mixed.reshape(props, seqs, feats)),
        root.reshape(base_state.shape),
        major(next_v), major(next_b), major(next_c),
        major(next_s.reshape(props, seqs, heads)),
    )


def solution(mesh):
    split = P("kv", None, "tp")
    weight = P("kv", "tp")
    state = P("kv", "tp", None, None)
    return jax.shard_map(
        on_device,
        mesh=mesh,
        in_specs=(
            split, P(), weight, weight, weight, weight, P(),
            P(None, "tp"), P(None, "tp"), P(None, "tp"),
            P("tp"), P("tp"), P("tp"), P("tp"),
            P("tp", "kv"),
            state, split, split, split, split, P("kv"),
        ),
        out_specs=(split, state, split, split, split, split),
        check_vma=False,
    )
```

```python
import functools
from typing import NamedTuple

import jax
import jax.numpy as jnp
from jax import lax
from jax.experimental import pallas as pl
from jax.experimental.pallas import tpu as pltpu
from jax.sharding import PartitionSpec as P

STATE_DIM = 128
LANES = 128
SMALL = 21
EPSILON = 1e-06
MESH = pl.DeviceIdType.MESH
F32 = jnp.float32
BF16 = jnp.bfloat16


class Dims(NamedTuple):
    far: int
    near: int
    n_tp: int
    seqs: int
    props: int
    taps: int
    width: int
    feats: int
    depth: int
    groups: int
    gw: int
    heads: int
    out_cols: int

    @property
    def rows(self):
        return self.seqs * self.props

    @property
    def n_kv(self):
        return self.far * self.near

    @property
    def block(self):
        return self.near * self.depth

    @property
    def part(self):
        return self.gw // self.near

    @property
    def every(self):
        return self.near // 2

    def thin(self, g):
        return g % self.every == 0

    def cols(self, g):
        return 2 * self.part + (STATE_DIM if self.thin(g) else 0)


def near_size(n_kv, gw):
    return max(
        d
        for d in range(2, n_kv + 1, 2)
        if n_kv % d == 0 and d * d <= n_kv and gw % (LANES * d) == 0
    )


def remote(src, dst, send, recv, kv, tp):
    return pltpu.make_async_remote_copy(
        src_ref=src,
        dst_ref=dst,
        send_sem=send,
        recv_sem=recv,
        device_id={"kv": kv, "tp": tp},
        device_id_type=MESH,
    )


def silu(v):
    return v / (1.0 + jnp.exp(-v))


def softplus(v):
    return jnp.maximum(v, 0.0) + jnp.log1p(jnp.exp(-jnp.abs(v)))


def conv(rows, taps, count):
    out = []
    for t in range(count):
        total = taps[0] * rows[t]
        for k in range(1, len(taps)):
            total = total + taps[k] * rows[t + k]
        out.append(total)
    return out


NT = (((1,), (1,)), ((), ()))


def mixer_kernel(d, *refs):
    gate_w, value_w, write_w, read_w, wout_h, base_h = refs[:6]
    small = refs[6:SMALL]
    mixed, base_v, next_v, next_b, next_c, next_s = refs[SMALL : SMALL + 6]
    rest = list(refs[SMALL + 6 :])
    G = d.groups
    stage, wbuf, zmine, zin, red, back, rootb, ys = (rest[i * G : (i + 1) * G] for i in range(8))
    (
        xq, xs, pt_mine, pt_in, wout, acc, mine, parts,
        ssem, w_sem, xz_sem, xp_sem, pt_sem, z_sem, b_sem, y_sem, m_sem, l_sem,
    ) = rest[8 * G : 8 * G + 18]
    held = rest[8 * G + 18 :]
    (
        tok, gain, step_w, conv_v, conv_b, conv_c, bias_r, decay_r, skip_r, gain_out,
        past_v, past_b, past_c, past_s, taken_ref,
    ) = held
    far, near, n_tp, rows, S, N = d.far, d.near, d.n_tp, d.rows, d.seqs, STATE_DIM
    n_kv, part, gw, props = d.n_kv, d.part, d.gw, d.props
    me, tp = lax.axis_index("kv"), lax.axis_index("tp")
    h, l = lax.div(me, near), lax.rem(me, near)

    barrier = pltpu.get_barrier_semaphore()

    def greet(kv, t):
        pl.semaphore_signal(barrier, inc=1, device_id={"kv": kv, "tp": t}, device_id_type=MESH)

    for step in range(1, near):
        greet(h * near + lax.rem(l + step, near), tp)
    for t in range(n_tp):
        for step in range(1, far):
            greet(lax.rem(h + step, far) * near + l, t)
    for step in range(1, n_tp):
        greet(me, lax.rem(tp + step, n_tp))
    greeted = near - 1 + (far - 1) * n_tp + n_tp - 1

    class Mark:
        scope = None

        def __call__(self, name):
            if self.scope is not None:
                self.scope.__exit__(None, None, None)
            self.scope = None
            if name is not None:
                self.scope = jax.named_scope(name)
                self.scope.__enter__()

    mark = Mark()
    mark("prologue")
    used = []

    def local(src, dst):
        copy = pltpu.make_async_copy(src, dst, l_sem.at[len(used)])
        copy.start()
        used.append(copy)
        return copy

    fetch = [local(src, dst) for src, dst in zip(small, held)]
    units = 2 * G
    staging = []
    for g in range(G):
        copies = []
        for k in range(near):
            lo = g * gw + k * part
            copies.append(local(gate_w.at[:, lo : lo + part], stage[g].at[k, :, 0:part]))
            copies.append(local(value_w.at[:, lo : lo + part], stage[g].at[k, :, part : 2 * part]))
            if d.thin(g):
                u = (g // d.every * near + k) % units
                source = (write_w, read_w)[u % 2]
                copies.append(
                    local(
                        source.at[:, u // 2 * N : (u // 2 + 1) * N],
                        stage[g].at[k, :, 2 * part : 2 * part + N],
                    )
                )
        staging.append(copies)
    loading = [
        local(base_h.at[:, g * gw : (g + 1) * gw], base_v.at[:, g * gw : (g + 1) * gw])
        for g in range(G)
    ]
    wout_load = local(wout_h, wout)

    sends = []

    def send(src, dst, recv, kv, t, cond=None):
        copy = remote(src, dst, ssem.at[len(sends)], recv, kv, t)
        sends.append((copy, cond))
        if cond is None:
            copy.start()
        else:
            pl.when(cond)(copy.start)

    def arrive(dst, recv, cond=None):
        copy = remote(dst, dst, ssem.at[0], recv, me, tp)
        if cond is None:
            copy.wait_recv()
        else:
            pl.when(cond)(copy.wait_recv)

    nb = d.feats // d.block
    own = pl.multiple_of(tp * d.feats, d.feats)
    for copy in fetch:
        copy.wait()
    order = lax.broadcasted_iota(jnp.int32, (rows, rows), 0)
    other = lax.broadcasted_iota(jnp.int32, (rows, rows), 1)

    def shuffle(major, minor):
        source = lax.rem(order, minor) * major + lax.div(order, minor)
        return jnp.where(other == source, 1.0, 0.0).astype(BF16)

    to_time, to_seq = shuffle(props, S), shuffle(S, props)

    def time_major(ref):
        stacked = jnp.concatenate([ref[s].astype(F32) for s in range(S)], axis=0).astype(BF16)
        return jnp.dot(to_time, stacked, preferred_element_type=F32)

    def put_seq(ref, cols, value):
        value = jnp.dot(to_seq, value, preferred_element_type=F32)
        for s in range(S):
            ref[s, :, cols] = value[s * props : (s + 1) * props].astype(BF16)

    raw = time_major(tok)
    square = jnp.sum(raw * raw, axis=-1, keepdims=True)
    scaled = (raw * gain[:, pl.ds(own, d.feats)]).astype(BF16)
    for q in range(nb):
        xq[q] = scaled[:, q * d.block : (q + 1) * d.block]
    hpad = pt_mine.shape[2] - LANES
    for t in range(n_tp):
        term = lax.dot_general(
            scaled, step_w[t * d.heads : (t + 1) * d.heads, pl.ds(own, d.feats)], NT,
            preferred_element_type=F32,
        )
        pt_mine[t, :, 0 : d.heads] = term
        pt_mine[t, :, hpad : hpad + LANES] = jnp.broadcast_to(square, (rows, LANES))
    pt_in[tp] = pt_mine[tp]

    mark('barrier')
    pl.semaphore_wait(barrier, greeted)

    mark('tok_send')
    home = lax.div(h, nb)
    for q in range(nb):
        plane = tp * nb + q
        for t in range(n_tp):
            away = jnp.logical_or(plane != h, tp != t)
            send(xq.at[q], xs.at[l, h], xz_sem.at[h], plane * near + l, t, away)

    @pl.when(home == tp)
    def _():
        xs[l, h] = xq[lax.rem(h, nb)]

    for step in range(1, n_tp):
        t = lax.rem(tp + step, n_tp)
        send(pt_mine.at[t], pt_in.at[tp], pt_sem.at[tp], me, t)

    def send_weights(g):
        for copy in staging[g]:
            copy.wait()
        for step in range(1, near):
            k = lax.rem(l + step, near)
            send(stage[g].at[k], wbuf[g].at[l], w_sem.at[g, l], h * near + k, tp)

    send_weights(0)

    diagonal = lax.broadcasted_iota(jnp.int32, (S, S), 0) == lax.broadcasted_iota(
        jnp.int32, (S, S), 1
    )
    taken = jnp.sum(
        jnp.where(diagonal, taken_ref[...].astype(F32), 0.0), axis=-1, keepdims=True
    ).astype(jnp.int32)
    steps_old = time_major(past_s).astype(BF16)
    head_rows = jnp.concatenate(
        [bias_r[...], decay_r[...], skip_r[...]] + [jnp.zeros_like(bias_r[...])] * 5, axis=0
    )
    params = []
    row_seq = lax.rem(lax.broadcasted_iota(jnp.int32, (rows, N), 0), S)

    def spread(g):
        r = lax.broadcasted_iota(jnp.int32, (d.heads, gw), 0)
        c = lax.broadcasted_iota(jnp.int32, (d.heads, gw), 1)
        hw = gw * G // d.heads
        lo = r * hw - g * gw
        return jnp.where(jnp.logical_and(c >= lo, c < lo + hw), 1.0, 0.0).astype(BF16)

    def span(g, w):
        return slice(g * w, (g + 1) * w)

    def taps(ref, cols):
        return [ref[k : k + 1, cols] for k in range(d.taps)]

    def param(k, g):
        if g == len(params):
            params.append(
                jnp.dot(
                    head_rows, spread(g).astype(F32), preferred_element_type=F32,
                    precision=lax.Precision.HIGHEST,
                )
            )
        return params[g][k : k + 1]

    def pieces(v):
        return [v[t * S : (t + 1) * S] for t in range(props)]

    def old(ref, cols):
        return [ref[i, :, cols].astype(F32) for i in range(ref.shape[0])]

    def root(g):
        mark(f'root{g}')
        loading[g].wait()
        cv, cn = span(g, gw), span(g, N)
        px = [silu(v) for v in conv(old(past_v, cv), taps(conv_v, cv), props)]
        pb = [silu(v) for v in conv(old(past_b, cn), taps(conv_b, cn), props)]
        pd = softplus(
            jnp.dot(steps_old, spread(g), preferred_element_type=F32) + param(0, g)
        )
        rate = jnp.exp(param(1, g))
        pd = pieces(pd)
        log = [jnp.where(taken > t, -rate * pd[t], 0.0) for t in range(props)]
        tail = jnp.zeros_like(log[0])
        weighted = [None] * props
        for t in reversed(range(props)):
            weighted[t] = jnp.where(taken > t, jnp.exp(tail) * pd[t], 0.0) * px[t]
            tail = tail + log[t]
        left = jnp.transpose(jnp.concatenate(weighted, axis=0)).astype(BF16)
        decay = jnp.exp(tail)
        fill = [decay] * max(1, 8 // S)
        decay = jnp.transpose(jnp.concatenate(fill, axis=0))
        right = jnp.concatenate(pb, axis=0)
        for s in range(S):
            outer = jnp.dot(
                left,
                jnp.where(row_seq == s, right, 0.0).astype(BF16),
                preferred_element_type=F32,
            )
            new = decay[:, s : s + 1] * base_v[s, cv, :] + outer
            base_v[s, cv, :] = new
            rootb[g][:, span(s, N)] = new.astype(BF16)

    root(0)

    mark('tokz_wait')
    for k in range(far):
        arrive(
            xs.at[l, k], xz_sem.at[k], jnp.logical_or(h != k, home != tp)
        )
    for step in range(1, near):
        send(xs.at[l], xs.at[l], xp_sem.at[l], h * near + lax.rem(l + step, near), tp)
    for g in range(1, G):
        send_weights(g)

    mark('scale')
    for step in range(1, n_tp):
        t = lax.rem(tp + n_tp - step, n_tp)
        arrive(pt_in.at[t], pt_sem.at[t])
    joined = pt_in[0]
    for t in range(1, n_tp):
        joined = joined + pt_in[t]
    scale = lax.rsqrt(joined[:, hpad : hpad + LANES] * (1.0 / d.width) + EPSILON)
    step_now = (joined[:, 0 : d.heads] * scale[:, 0 : d.heads]).astype(BF16)
    put_seq(next_s, slice(None), step_now)

    mark('tokp_wait')
    for step in range(1, near):
        k = lax.rem(l + near - step, near)
        arrive(xs.at[k], xp_sem.at[k])

    def project(g):
        mark(f'w_wait{g}')
        wbuf[g][l] = stage[g][l]
        for step in range(1, near):
            k = lax.rem(l + near - step, near)
            arrive(wbuf[g].at[k], w_sem.at[g, k])
        mark(f'matmul{g}')
        cols = d.cols(g)
        product = jnp.dot(
            xs[...].reshape(n_kv * rows, d.block),
            wbuf[g][...].reshape(d.block, cols),
            preferred_element_type=F32,
        ).astype(BF16)
        for k in range(near):
            for z in range(far):
                at = (k * far + z) * rows
                zmine[g][z, k] = product[at : at + rows]
        for step in range(1, far):
            z = lax.rem(h + step, far)
            send(zmine[g].at[z], zin[g].at[h], z_sem.at[g, h], z * near + l, tp)

    def collect(g):
        mark(f'z_wait{g}')
        value = zmine[g][h].astype(F32)
        for step in range(1, far):
            z = lax.rem(h + far - step, far)
            arrive(zin[g].at[z], z_sem.at[g, z])
            value = value + zin[g][z].astype(F32)
        red[g][...] = value.astype(BF16)
        back[g][l] = red[g][l]
        for step in range(1, near):
            k = lax.rem(l + step, near)
            send(red[g].at[k], back[g].at[l], b_sem.at[g, l], h * near + k, tp)

    def rounded(piece):
        return (piece.astype(F32) * scale).astype(BF16).astype(F32)

    def advance(g):
        mark(f'b_wait{g}')
        for step in range(1, near):
            k = lax.rem(l + near - step, near)
            arrive(back[g].at[k], b_sem.at[g, k])
        cv, cn = span(g, gw), span(g, N)
        mark(f'advance{g}')
        gate = jnp.concatenate([rounded(back[g][k, :, 0:part]) for k in range(near)], axis=1)
        value = jnp.concatenate(
            [rounded(back[g][k, :, part : 2 * part]) for k in range(near)], axis=1
        )

        def unit(u):
            j, k = u // near, u % near
            return rounded(back[j * d.every][k, :, 2 * part : 2 * part + N])

        def window(past, now, out, cols):
            before = old(past, cols)
            rows_now = []
            for i in range(d.taps - 1):
                row = before[i + 1]
                for a in range(2, props + 1):
                    row = jnp.where(taken == a, before[i + a], row)
                rows_now.append(row)
            rows_now = rows_now + pieces(now)
            for i, row in enumerate(rows_now):
                out[i, :, cols] = row.astype(BF16)
            return rows_now

        win_v = window(past_v, value, next_v, cv)
        win_b = window(past_b, unit(2 * g), next_b, cn)
        win_c = window(past_c, unit(2 * g + 1), next_c, cn)
        x = [silu(v) for v in conv(win_v, taps(conv_v, cv), props)]
        b = [silu(v) for v in conv(win_b, taps(conv_b, cn), props)]
        c = [silu(v) for v in conv(win_c, taps(conv_c, cn), props)]
        whole = jnp.concatenate(c, axis=0)
        masked = jnp.concatenate(
            [jnp.where(row_seq == s, whole, 0.0) for s in range(S)], axis=1
        ).astype(BF16)
        carried = pieces(
            lax.dot_general(masked, rootb[g][...], NT, preferred_element_type=F32)
        )
        dt = pieces(
            softplus(jnp.dot(step_now, spread(g), preferred_element_type=F32) + param(0, g))
        )
        rate = jnp.exp(param(1, g))
        logs = []
        for t in range(props):
            log = -rate * dt[t]
            logs.append(log if t == 0 else logs[-1] + log)
        y = []
        for t in range(props):
            row = jnp.exp(logs[t]) * carried[t] + param(2, g) * x[t]
            for s in range(t + 1):
                score = jnp.sum(c[t] * b[s], axis=-1, keepdims=True)
                weight = dt[s] if s == t else jnp.exp(logs[t] - logs[s]) * dt[s]
                row = row + (score * weight) * x[s]
            y.append(row)
        gated = jnp.concatenate(y, axis=0) * silu(gate)
        mean = jnp.sum(gated * gated, axis=-1, keepdims=True) * (1.0 / gw)
        ys[g][me] = (gated * lax.rsqrt(mean + EPSILON) * gain_out[:, cv]).astype(BF16)
        for step in range(1, far):
            z = lax.rem(h + step, far)
            send(ys[g].at[me], ys[g].at[me], y_sem.at[g, me], z * near + l, tp)
        for step in range(1, near):
            k = lax.rem(l + step, near)
            send(ys[g].at[me], ys[g].at[me], y_sem.at[g, me], h * near + k, tp)

    def forward(g):
        mark(f'yz_wait{g}')
        for step in range(1, far):
            block = lax.rem(h + far - step, far) * near + l
            arrive(ys[g].at[block], y_sem.at[g, block])
            for side in range(1, near):
                k = lax.rem(l + side, near)
                send(ys[g].at[block], ys[g].at[block], y_sem.at[g, block], h * near + k, tp)

    def output(g):
        mark(f'y_wait{g}')
        for side in range(1, near):
            k = lax.rem(l + near - side, near)
            for step in range(far):
                block = lax.rem(h + far - step, far) * near + k
                arrive(ys[g].at[block], y_sem.at[g, block])
        if g == 0:
            wout_load.wait()
        mark(f'out{g}')
        term = jnp.dot(
            ys[g][...].reshape(n_kv * rows, gw), wout[span(g, gw), :], preferred_element_type=F32
        )
        if g == 0:
            acc[...] = term
        else:
            acc[...] += term

    stages = (
        (project, 0.0), (collect, 5.0), (advance, 9.0), (forward, 13.0), (output, 25.0),
    )
    order_of = sorted(
        (start + 3.3 * g, i, g) for i, (_, start) in enumerate(stages) for g in range(G)
    )
    for _, i, g in order_of:
        stages[i][0](g)
        if i == 0 and g + 1 < G:
            root(g + 1)

    mark('final_send')
    cols = d.out_cols
    mine[...] = acc[...].astype(BF16).reshape(n_kv, rows, cols)
    per = n_kv // n_tp
    side, place = lax.div(me, per), lax.rem(me, per)
    for step in range(n_kv):
        k = lax.rem(me + step, n_kv)
        send(
            mine.at[k], parts.at[tp, place], m_sem.at[tp, place], k, side,
            (side != tp) if step == 0 else None,
        )

    @pl.when(side == tp)
    def _():
        parts[tp, place] = mine[me]

    mark('final_wait')
    for t in range(n_tp):
        for k in range(per):
            arrive(
                parts.at[t, k], m_sem.at[t, k], jnp.logical_or(t != tp, tp * per + k != me)
            )
    for k in range(per):
        value = parts[0, k].astype(F32)
        for t in range(1, n_tp):
            value = value + parts[t, k].astype(F32)
        put_seq(mixed, span(k, cols), value.astype(BF16))
    mark('drain')
    for copy, cond in sends:
        if cond is None:
            copy.wait_send()
        else:
            pl.when(cond)(copy.wait_send)
    mark(None)


def mixer(d, args):
    G, near, far, rows, n_kv = d.groups, d.near, d.far, d.rows, d.n_kv
    dma = pltpu.SemaphoreType.DMA
    vmem, hbm = pl.BlockSpec(memory_space=pltpu.VMEM), pl.BlockSpec(memory_space=pltpu.HBM)

    def each(shape):
        return [pltpu.VMEM(shape(g), BF16) for g in range(G)]

    scratch = (
        each(lambda g: (near, d.depth, d.cols(g)))
        + each(lambda g: (near, d.depth, d.cols(g)))
        + each(lambda g: (far, near, rows, d.cols(g)))
        + each(lambda g: (far, near, rows, d.cols(g)))
        + each(lambda g: (near, rows, d.cols(g)))
        + each(lambda g: (near, rows, d.cols(g)))
        + each(lambda g: (d.gw, d.seqs * STATE_DIM))
        + each(lambda g: (n_kv, rows, d.gw))
    )
    nb = d.feats // d.block
    hpad = -(-d.heads // LANES) * LANES
    per = n_kv // d.n_tp
    n_send = (
        nb * d.n_tp + d.n_tp - 1 + near - 1
        + G * (2 * (near - 1) + far - 1)
        + G * (far - 1 + (near - 1) * far)
        + n_kv
    )
    n_local = sum(near * (3 if d.thin(g) else 2) for g in range(G)) + G + 1 + len(args) - 6
    scratch = scratch + [
        pltpu.VMEM((nb, rows, d.block), BF16),
        pltpu.VMEM((near, far, rows, d.block), BF16),
        pltpu.VMEM((d.n_tp, rows, hpad + LANES), F32),
        pltpu.VMEM((d.n_tp, rows, hpad + LANES), F32),
        pltpu.VMEM((G * d.gw, d.out_cols), BF16),
        pltpu.VMEM((n_kv * rows, d.out_cols), F32),
        pltpu.VMEM((n_kv, rows, d.out_cols), BF16),
        pltpu.VMEM((d.n_tp, per, rows, d.out_cols), BF16),
        dma((n_send,)), dma((G, near)), dma((far,)), dma((near,)), dma((d.n_tp,)),
        dma((G, far)), dma((G, near)), dma((G, n_kv)), dma((d.n_tp, per)), dma((n_local,)),
    ]
    scratch = scratch + [pltpu.VMEM(item.shape, item.dtype) for item in args[6:]]
    past_v, past_b, past_c = (item.shape for item in args[-5:-2])
    return pl.pallas_call(
        functools.partial(mixer_kernel, d),
        out_shape=[
            pltpu.VMEM((d.seqs, d.props, d.feats), BF16),
            pltpu.VMEM((d.seqs, G * d.gw, STATE_DIM), F32),
            pltpu.VMEM(past_v, BF16),
            pltpu.VMEM(past_b, BF16),
            pltpu.VMEM(past_c, BF16),
            pltpu.VMEM((d.seqs, d.props, d.heads), BF16),
        ],
        in_specs=[hbm] * len(args),
        out_specs=[vmem] * 6,
        scratch_shapes=scratch,
        compiler_params=pltpu.CompilerParams(
            collective_id=0, has_side_effects=True, vmem_limit_bytes=24 * 2**20
        ),
        name="mixer",
    )(*(pltpu.with_memory_space_constraint(item, pltpu.HBM) for item in args))


def store_kernel(count, *refs):
    sem = refs[-1]
    copies = [
        pltpu.make_async_copy(refs[i], refs[count + i], sem.at[i]) for i in range(count)
    ]
    for copy in copies:
        copy.start()
    for copy in copies:
        copy.wait()


def store(items):
    count = len(items)
    return pl.pallas_call(
        functools.partial(store_kernel, count),
        out_shape=[jax.ShapeDtypeStruct(item.shape, item.dtype) for item in items],
        in_specs=[pl.BlockSpec(memory_space=pltpu.VMEM)] * count,
        out_specs=[pl.BlockSpec(memory_space=pltpu.HBM)] * count,
        scratch_shapes=[pltpu.SemaphoreType.DMA((count,))],
        compiler_params=pltpu.CompilerParams(vmem_limit_bytes=2**20),
        name="store",
    )(*items)


def on_device(
    tokens, input_gain, gate_weight, value_weight, write_weight, read_weight, step_weight,
    conv_value, conv_write, conv_read, step_bias, decay_log, skip_gain, output_gain, out_weight,
    base_state, past_value, past_write, past_read, past_step, accepted,
):
    seqs, props, feats = tokens.shape
    n_kv, n_tp = lax.axis_size("kv"), lax.axis_size("tp")
    depth, inner = gate_weight.shape
    groups = write_weight.shape[1] // STATE_DIM
    heads = step_bias.shape[0]
    gw = inner // groups
    near = near_size(n_kv, gw)
    d = Dims(
        far=n_kv // near, near=near, n_tp=n_tp, seqs=seqs, props=props,
        taps=conv_value.shape[0], width=feats * n_tp, feats=feats, depth=depth, groups=groups,
        gw=gw, heads=heads, out_cols=out_weight.shape[1],
    )

    def major(item):
        return item.transpose(1, 0, 2)

    def line(item):
        return item.reshape(1, item.shape[0])

    outs = mixer(
        d,
        (
            gate_weight, value_weight, write_weight, read_weight, out_weight,
            base_state.reshape(seqs, inner, STATE_DIM),
            tokens, line(input_gain), step_weight.T, conv_value, conv_write, conv_read,
            line(step_bias), line(decay_log), line(skip_gain), line(output_gain),
            major(past_value), major(past_write), major(past_read), past_step, line(accepted),
        ),
    )
    mixed, root, next_v, next_b, next_c, next_s = store(outs)
    return (
        mixed, root.reshape(base_state.shape), major(next_v), major(next_b), major(next_c), next_s,
    )


def solution(mesh):
    split = P("kv", None, "tp")
    weight = P("kv", "tp")
    state = P("kv", "tp", None, None)
    return jax.shard_map(
        on_device,
        mesh=mesh,
        in_specs=(
            split, P(), weight, weight, weight, weight, P(),
            P(None, "tp"), P(None, "tp"), P(None, "tp"),
            P("tp"), P("tp"), P("tp"), P("tp"),
            P("tp", "kv"),
            state, split, split, split, split, P("kv"),
        ),
        out_specs=(split, state, split, split, split, split),
        check_vma=False,
    )
```

```python
import functools
from typing import NamedTuple

import jax
import jax.numpy as jnp
from jax import lax
from jax.experimental import pallas as pl
from jax.experimental.pallas import tpu as pltpu
from jax.sharding import PartitionSpec as P

STATE_DIM = 128
LANES = 128
SMALL = 21
EPSILON = 1e-06
MESH = pl.DeviceIdType.MESH
F32 = jnp.float32
BF16 = jnp.bfloat16


class Dims(NamedTuple):
    far: int
    near: int
    n_tp: int
    seqs: int
    props: int
    taps: int
    width: int
    feats: int
    depth: int
    groups: int
    gw: int
    heads: int
    out_cols: int

    @property
    def rows(self):
        return self.seqs * self.props

    @property
    def n_kv(self):
        return self.far * self.near

    @property
    def block(self):
        return self.near * self.depth

    @property
    def part(self):
        return self.gw // self.near

    def thin(self, g):
        return g * self.near < 2 * self.groups

    def cols(self, g):
        return 2 * self.part + (STATE_DIM if self.thin(g) else 0)


def near_size(n_kv, gw):
    return max(
        d
        for d in range(2, n_kv + 1, 2)
        if n_kv % d == 0 and d * d <= n_kv and gw % (LANES * d) == 0
    )


def remote(src, dst, send, recv, kv, tp):
    return pltpu.make_async_remote_copy(
        src_ref=src,
        dst_ref=dst,
        send_sem=send,
        recv_sem=recv,
        device_id={"kv": kv, "tp": tp},
        device_id_type=MESH,
    )


def silu(v):
    return v / (1.0 + jnp.exp(-v))


def softplus(v):
    return jnp.maximum(v, 0.0) + jnp.log1p(jnp.exp(-jnp.abs(v)))


def conv(rows, taps, count):
    out = []
    for t in range(count):
        total = taps[0] * rows[t]
        for k in range(1, len(taps)):
            total = total + taps[k] * rows[t + k]
        out.append(total)
    return out


NT = (((1,), (1,)), ((), ()))


def mixer_kernel(d, *refs):
    gate_w, value_w, write_w, read_w, wout_h, base_h = refs[:6]
    small = refs[6:SMALL]
    mixed, base_v, next_v, next_b, next_c, next_s = refs[SMALL : SMALL + 6]
    rest = list(refs[SMALL + 6 :])
    G = d.groups
    stage, wbuf, zmine, zin, red, back, rootb = (rest[i * G : (i + 1) * G] for i in range(7))
    ys, rest = rest[7 * G : 8 * G - 1], rest[8 * G - 1 :]
    last = G - 1
    (
        xq, xs, pt_mine, pt_in, wout, acc, mine, parts, wlast, ylast, mine_l, parts_l,
        ssem, w_sem, xz_sem, xp_sem, pt_sem, z_sem, b_sem, yz_sem, yp_sem, m_sem,
        wl_sem, yl_sem, ml_sem, l_sem, g_sem,
    ) = rest[:27]
    held = rest[27:]
    (
        tok, gain, step_w, conv_v, conv_b, conv_c, bias_r, decay_r, skip_r, gain_out,
        past_v, past_b, past_c, past_s, taken_ref,
    ) = held
    far, near, n_tp, rows, S, N = d.far, d.near, d.n_tp, d.rows, d.seqs, STATE_DIM
    n_kv, part, gw, props = d.n_kv, d.part, d.gw, d.props
    me, tp = lax.axis_index("kv"), lax.axis_index("tp")
    h, l = lax.div(me, near), lax.rem(me, near)

    barrier = pltpu.get_barrier_semaphore()

    def greet(kv, t):
        pl.semaphore_signal(barrier, inc=1, device_id={"kv": kv, "tp": t}, device_id_type=MESH)

    for step in range(1, near):
        greet(h * near + lax.rem(l + step, near), tp)
    for t in range(n_tp):
        for step in range(1, far):
            greet(lax.rem(h + step, far) * near + l, t)
    for step in range(1, n_tp):
        greet(me, lax.rem(tp + step, n_tp))
    greeted = near - 1 + (far - 1) * n_tp + n_tp - 1

    class Mark:
        scope = None

        def __call__(self, name):
            if self.scope is not None:
                self.scope.__exit__(None, None, None)
            self.scope = None
            if name is not None:
                self.scope = jax.named_scope(name)
                self.scope.__enter__()

    mark = Mark()
    mark("prologue")
    used = []

    def local(src, dst):
        copy = pltpu.make_async_copy(src, dst, l_sem.at[len(used)])
        copy.start()
        used.append(copy)
        return copy

    fetch = [local(src, dst) for src, dst in zip(small, held)]
    units = 2 * G
    for g in range(G):
        def stage_in(src, dst):
            pltpu.make_async_copy(src, dst, g_sem.at[g]).start()

        for k in range(near):
            lo = g * gw + k * part
            stage_in(gate_w.at[:, lo : lo + part], stage[g].at[k, :, 0:part])
            stage_in(value_w.at[:, lo : lo + part], stage[g].at[k, :, part : 2 * part])
            if d.thin(g):
                u = (g * near + k) % units
                source = (write_w, read_w)[u % 2]
                stage_in(
                    source.at[:, u // 2 * N : (u // 2 + 1) * N],
                    stage[g].at[k, :, 2 * part : 2 * part + N],
                )
    loading = [
        local(base_h.at[:, g * gw : (g + 1) * gw], base_v.at[:, g * gw : (g + 1) * gw])
        for g in range(G)
    ]
    wlast_load = local(wout_h.at[last * gw : G * gw], wlast.at[h])
    wout_load = local(wout_h, wout)

    drains = []

    def meter(ref, count):
        at = len(drains)
        size = ref if count is None else ref.at[pl.ds(0, count)]
        drains.append((size, at, None))
        return at

    def alone(src, cond=None):
        drains.append((src, len(drains), cond))
        return len(drains) - 1

    def send(src, dst, recv, kv, t, cond=None, via=None):
        at = alone(src, cond) if via is None else via
        copy = remote(src, dst, ssem.at[at], recv, kv, t)
        if cond is None:
            copy.start()
        else:
            pl.when(cond)(copy.start)

    def arrive(dst, recv, cond=None):
        copy = remote(dst, dst, ssem.at[0], recv, me, tp)
        if cond is None:
            copy.wait_recv()
        else:
            pl.when(cond)(copy.wait_recv)

    def first(ref, count):
        return ref.at[pl.ds(0, count)]

    nb = d.feats // d.block
    own = pl.multiple_of(tp * d.feats, d.feats)
    for copy in fetch:
        copy.wait()
    order = lax.broadcasted_iota(jnp.int32, (rows, rows), 0)
    other = lax.broadcasted_iota(jnp.int32, (rows, rows), 1)

    def shuffle(major, minor):
        source = lax.rem(order, minor) * major + lax.div(order, minor)
        return jnp.where(other == source, 1.0, 0.0).astype(BF16)

    to_time, to_seq = shuffle(props, S), shuffle(S, props)

    def time_major(ref):
        stacked = jnp.concatenate([ref[s].astype(F32) for s in range(S)], axis=0).astype(BF16)
        return jnp.dot(to_time, stacked, preferred_element_type=F32)

    def put_seq(ref, cols, value):
        value = jnp.dot(to_seq, value, preferred_element_type=F32)
        for s in range(S):
            ref[s, :, cols] = value[s * props : (s + 1) * props].astype(BF16)

    raw = time_major(tok)
    square = jnp.sum(raw * raw, axis=-1, keepdims=True)
    scaled = (raw * gain[:, pl.ds(own, d.feats)]).astype(BF16)
    for q in range(nb):
        xq[q] = scaled[:, q * d.block : (q + 1) * d.block]
    hpad = pt_mine.shape[2] - LANES
    for t in range(n_tp):
        term = lax.dot_general(
            scaled, step_w[t * d.heads : (t + 1) * d.heads, pl.ds(own, d.feats)], NT,
            preferred_element_type=F32,
        )
        pt_mine[t, :, 0 : d.heads] = term
        pt_mine[t, :, hpad : hpad + LANES] = jnp.broadcast_to(square, (rows, LANES))
    pt_in[tp] = pt_mine[tp]

    mark('barrier')
    pl.semaphore_wait(barrier, greeted)

    mark('tok_send')
    home = lax.div(h, nb)
    for q in range(nb):
        plane = tp * nb + q
        for t in range(n_tp):
            away = jnp.logical_or(plane != h, tp != t)
            send(xq.at[q], xs.at[l, h], xz_sem.at[h], plane * near + l, t, away)

    @pl.when(home == tp)
    def _():
        xs[l, h] = xq[lax.rem(h, nb)]

    for step in range(1, n_tp):
        t = lax.rem(tp + step, n_tp)
        send(pt_mine.at[t], pt_in.at[tp], pt_sem.at[tp], me, t)

    def send_weights(g):
        arrive(stage[g], g_sem.at[g])
        via = meter(stage[g], near - 1)
        for step in range(1, near):
            k = lax.rem(l + step, near)
            send(stage[g].at[k], wbuf[g].at[l], w_sem.at[g], h * near + k, tp, via=via)

    send_weights(0)
    wlast_load.wait()

    def inside(z):
        return jnp.logical_and(z >= 0, z < far)

    def relay(level):
        for way in (1, -1):
            z = h - way * level
            block = lax.rem(z + far, far)
            if level:
                arrive(wlast.at[block], wl_sem.at[block], inside(z))
            if level < far - 1:
                peer = lax.rem(h + way + far, far) * near + l
                go = jnp.logical_and(inside(z), inside(h + way))
                send(wlast.at[block], wlast.at[block], wl_sem.at[block], peer, tp, go)

    diagonal = lax.broadcasted_iota(jnp.int32, (S, S), 0) == lax.broadcasted_iota(
        jnp.int32, (S, S), 1
    )
    taken = jnp.sum(
        jnp.where(diagonal, taken_ref[...].astype(F32), 0.0), axis=-1, keepdims=True
    ).astype(jnp.int32)
    steps_old = time_major(past_s).astype(BF16)
    head_rows = jnp.concatenate(
        [bias_r[...], decay_r[...], skip_r[...]] + [jnp.zeros_like(bias_r[...])] * 5, axis=0
    )
    params = []
    row_seq = lax.rem(lax.broadcasted_iota(jnp.int32, (rows, N), 0), S)

    def spread(g):
        r = lax.broadcasted_iota(jnp.int32, (d.heads, gw), 0)
        c = lax.broadcasted_iota(jnp.int32, (d.heads, gw), 1)
        hw = gw * G // d.heads
        lo = r * hw - g * gw
        return jnp.where(jnp.logical_and(c >= lo, c < lo + hw), 1.0, 0.0).astype(BF16)

    def span(g, w):
        return slice(g * w, (g + 1) * w)

    def taps(ref, cols):
        return [ref[k : k + 1, cols] for k in range(d.taps)]

    def param(k, g):
        if g == len(params):
            params.append(
                jnp.dot(
                    head_rows, spread(g).astype(F32), preferred_element_type=F32,
                    precision=lax.Precision.HIGHEST,
                )
            )
        return params[g][k : k + 1]

    def pieces(v):
        return [v[t * S : (t + 1) * S] for t in range(props)]

    def old(ref, cols):
        return [ref[i, :, cols].astype(F32) for i in range(ref.shape[0])]

    def root(g):
        mark(f'root{g}')
        loading[g].wait()
        cv, cn = span(g, gw), span(g, N)
        px = [silu(v) for v in conv(old(past_v, cv), taps(conv_v, cv), props)]
        pb = [silu(v) for v in conv(old(past_b, cn), taps(conv_b, cn), props)]
        pd = softplus(
            jnp.dot(steps_old, spread(g), preferred_element_type=F32) + param(0, g)
        )
        rate = jnp.exp(param(1, g))
        pd = pieces(pd)
        log = [jnp.where(taken > t, -rate * pd[t], 0.0) for t in range(props)]
        tail = jnp.zeros_like(log[0])
        weighted = [None] * props
        for t in reversed(range(props)):
            weighted[t] = jnp.where(taken > t, jnp.exp(tail) * pd[t], 0.0) * px[t]
            tail = tail + log[t]
        left = jnp.transpose(jnp.concatenate(weighted, axis=0)).astype(BF16)
        decay = jnp.exp(tail)
        fill = [decay] * max(1, 8 // S)
        decay = jnp.transpose(jnp.concatenate(fill, axis=0))
        right = jnp.concatenate(pb, axis=0)
        for s in range(S):
            outer = jnp.dot(
                left,
                jnp.where(row_seq == s, right, 0.0).astype(BF16),
                preferred_element_type=F32,
            )
            new = decay[:, s : s + 1] * base_v[s, cv, :] + outer
            base_v[s, cv, :] = new
            rootb[g][:, span(s, N)] = new.astype(BF16)

    for g in range(max(1, G - 1)):
        root(g)

    mark('tokz_wait')
    for k in range(far):
        arrive(
            xs.at[l, k], xz_sem.at[k], jnp.logical_or(h != k, home != tp)
        )
    fq = far // n_tp

    def piece(k, t):
        return xs.at[k, pl.ds(t * fq, fq)]

    via_x = meter(xs, near - 1)
    for step in range(1, near):
        k = h * near + lax.rem(l + step, near)
        send(piece(l, tp), piece(l, tp), xp_sem.at[l, tp], k, tp, via=via_x)
    for g in range(1, G):
        send_weights(g)
    relay(0)
    if G > 1:
        root(G - 1)

    mark('scale')
    for step in range(1, n_tp):
        t = lax.rem(tp + n_tp - step, n_tp)
        arrive(pt_in.at[t], pt_sem.at[t])
    joined = pt_in[0]
    for t in range(1, n_tp):
        joined = joined + pt_in[t]
    scale = lax.rsqrt(joined[:, hpad : hpad + LANES] * (1.0 / d.width) + EPSILON)
    step_now = (joined[:, 0 : d.heads] * scale[:, 0 : d.heads]).astype(BF16)
    put_seq(next_s, slice(None), step_now)

    mark('tokp_wait')
    for step in range(1, near):
        k = lax.rem(l + near - step, near)
        arrive(piece(k, tp), xp_sem.at[k, tp])
        for side in range(1, n_tp):
            t = lax.rem(tp + side, n_tp)
            send(piece(k, tp), piece(k, tp), xp_sem.at[k, tp], me, t, via=via_x)
    for step in range(1, near):
        k = lax.rem(l + near - step, near)
        for side in range(1, n_tp):
            t = lax.rem(tp + n_tp - side, n_tp)
            arrive(piece(k, t), xp_sem.at[k, t])

    def project(g):
        mark(f'w_wait{g}')
        wbuf[g][l] = stage[g][l]
        arrive(first(wbuf[g], near - 1), w_sem.at[g])
        mark(f'matmul{g}')
        cols = d.cols(g)
        product = jnp.dot(
            xs[...].reshape(n_kv * rows, d.block),
            wbuf[g][...].reshape(d.block, cols),
            preferred_element_type=F32,
        ).astype(BF16)
        for k in range(near):
            for z in range(far):
                at = (k * far + z) * rows
                zmine[g][z, k] = product[at : at + rows]
        via = meter(zmine[g], far - 1)
        for step in reversed(range(1, far)):
            z = lax.rem(h + step, far)
            send(zmine[g].at[z], zin[g].at[h], z_sem.at[g], z * near + l, tp, via=via)

    def collect(g):
        mark(f'z_wait{g}')
        arrive(first(zin[g], far - 1), z_sem.at[g])
        value = zmine[g][h].astype(F32)
        for step in range(1, far):
            z = lax.rem(h + far - step, far)
            value = value + zin[g][z].astype(F32)
        red[g][...] = value.astype(BF16)
        back[g][l] = red[g][l]
        via = meter(red[g], near - 1)
        for step in range(1, near):
            k = lax.rem(l + step, near)
            send(red[g].at[k], back[g].at[l], b_sem.at[g], h * near + k, tp, via=via)

    def rounded(piece):
        return (piece.astype(F32) * scale).astype(BF16).astype(F32)

    via_y = {}

    def advance(g):
        mark(f'b_wait{g}')
        arrive(first(back[g], near - 1), b_sem.at[g])
        cv, cn = span(g, gw), span(g, N)
        mark(f'advance{g}')
        gate = jnp.concatenate([rounded(back[g][k, :, 0:part]) for k in range(near)], axis=1)
        value = jnp.concatenate(
            [rounded(back[g][k, :, part : 2 * part]) for k in range(near)], axis=1
        )

        def unit(u):
            j, k = u // near, u % near
            return rounded(back[j][k, :, 2 * part : 2 * part + N])

        def window(past, now, out, cols):
            before = old(past, cols)
            rows_now = []
            for i in range(d.taps - 1):
                row = before[i + 1]
                for a in range(2, props + 1):
                    row = jnp.where(taken == a, before[i + a], row)
                rows_now.append(row)
            rows_now = rows_now + pieces(now)
            for i, row in enumerate(rows_now):
                out[i, :, cols] = row.astype(BF16)
            return rows_now

        win_v = window(past_v, value, next_v, cv)
        win_b = window(past_b, unit(2 * g), next_b, cn)
        win_c = window(past_c, unit(2 * g + 1), next_c, cn)
        x = [silu(v) for v in conv(win_v, taps(conv_v, cv), props)]
        b = [silu(v) for v in conv(win_b, taps(conv_b, cn), props)]
        c = [silu(v) for v in conv(win_c, taps(conv_c, cn), props)]
        whole = jnp.concatenate(c, axis=0)
        masked = jnp.concatenate(
            [jnp.where(row_seq == s, whole, 0.0) for s in range(S)], axis=1
        ).astype(BF16)
        carried = pieces(
            lax.dot_general(masked, rootb[g][...], NT, preferred_element_type=F32)
        )
        dt = pieces(
            softplus(jnp.dot(step_now, spread(g), preferred_element_type=F32) + param(0, g))
        )
        rate = jnp.exp(param(1, g))
        logs = []
        for t in range(props):
            log = -rate * dt[t]
            logs.append(log if t == 0 else logs[-1] + log)
        y = []
        for t in range(props):
            row = jnp.exp(logs[t]) * carried[t] + param(2, g) * x[t]
            for s in range(t + 1):
                score = jnp.sum(c[t] * b[s], axis=-1, keepdims=True)
                weight = dt[s] if s == t else jnp.exp(logs[t] - logs[s]) * dt[s]
                row = row + (score * weight) * x[s]
            y.append(row)
        gated = jnp.concatenate(y, axis=0) * silu(gate)
        mean = jnp.sum(gated * gated, axis=-1, keepdims=True) * (1.0 / gw)
        normal = (gated * lax.rsqrt(mean + EPSILON) * gain_out[:, cv]).astype(BF16)
        if g == last:
            ylast[l] = normal
            via = meter(ylast, near - 1)
            for step in range(1, near):
                k = lax.rem(l + step, near)
                send(ylast.at[l], ylast.at[l], yl_sem.at[0], h * near + k, tp, via=via)
            return
        ys[g][me] = normal
        via_y[g] = meter(ys[g], n_kv - 1)
        for step in reversed(range(1, far)):
            z = lax.rem(h + step, far)
            spot = ys[g].at[me]
            send(spot, spot, yz_sem.at[g], z * near + l, tp, via=via_y[g])
        for step in range(1, near):
            k = lax.rem(l + step, near)
            send(spot, spot, yp_sem.at[g], h * near + k, tp, via=via_y[g])

    def forward(g):
        mark(f'yz_wait{g}')
        arrive(first(ys[g], far - 1), yz_sem.at[g])
        for step in range(1, far):
            spot = ys[g].at[lax.rem(h + far - step, far) * near + l]
            for side in range(1, near):
                k = lax.rem(l + side, near)
                send(spot, spot, yp_sem.at[g], h * near + k, tp, via=via_y[g])

    def output(g):
        mark(f'y_wait{g}')
        arrive(first(ys[g], (near - 1) * far), yp_sem.at[g])
        if g == 0:
            wout_load.wait()
        mark(f'out{g}')
        term = jnp.dot(
            ys[g][...].reshape(n_kv * rows, gw), wout[span(g, gw), :], preferred_element_type=F32
        )
        if g == 0:
            acc[...] = term
        else:
            acc[...] += term

    cols = d.out_cols
    per = n_kv // n_tp
    side, place = lax.div(me, per), lax.rem(me, per)
    deep = per // near

    def share():
        mark('share')
        mine[...] = acc[...].astype(BF16).reshape(n_kv, rows, cols)
        via = meter(mine, n_kv - 1)
        slot = parts.at[tp * per + place]
        for step in range(1, n_kv):
            k = lax.rem(me + step, n_kv)
            send(mine.at[k], slot, m_sem.at[0], k, side, via=via)
        send(mine.at[me], slot, m_sem.at[0], me, side, side != tp)

        @pl.when(side == tp)
        def _():
            parts[tp * per + place] = mine[me]

    def output_last():
        mark('wl_wait')
        for level in levels:
            relay(level)
        if not last:
            wout_load.wait()
        mark('yl_wait')
        arrive(first(ylast, near - 1), yl_sem.at[0])
        mark('outl')
        every = ylast[...].reshape(near * rows, gw)
        for z in range(far):
            term = jnp.dot(every, wlast[z], preferred_element_type=F32).astype(BF16)
            for k in range(near):
                mine_l[z // deep * near + k, z % deep] = term[k * rows : (k + 1) * rows]
        via = meter(mine_l, near * n_tp - 1)
        spot = tp * near + l
        for step in range(1, near * n_tp):
            to = lax.rem(spot + step, near * n_tp)
            send(
                mine_l.at[to], parts_l.at[spot], ml_sem.at[0],
                h * near + lax.rem(to, near), lax.div(to, near), via=via,
            )
        parts_l[spot] = mine_l[spot]

    plan = (
        (project, lambda g: 2.75 * g),
        (collect, lambda g: 8.0 + 3.0 * g if g else 5.6),
        (advance, lambda g: 12.0 + 2.7 * g if g else 9.0),
        (forward, lambda g: 17.6 + 1.9 * g),
    )
    order_of = sorted(
        (when(g), i, g)
        for i, (_, when) in enumerate(plan)
        for g in range(G if i < 3 else last)
    )
    levels = iter(range(1, far))
    for _, i, g in order_of:
        plan[i][0](g)
        if far > 3 and g == last - 1 and i > 1:
            relay(next(levels))

    for g in range(last):
        output(g)
    if last:
        share()
    output_last()

    mark('final_wait')
    if last:
        arrive(first(parts, n_kv - 1), m_sem.at[0], side == tp)
        arrive(parts, m_sem.at[0], side != tp)
    mark('final_last')
    arrive(first(parts_l, near * n_tp - 1), ml_sem.at[0])
    for k in range(per):
        value = None
        for t in range(n_tp):
            terms = [parts_l[t * near + k % near, k // near]]
            terms = terms + ([parts[t * per + k]] if last else [])
            for term in terms:
                term = term.astype(F32)
                value = term if value is None else value + term
        put_seq(mixed, span(k, cols), value.astype(BF16))
    mark('drain')
    for size, at, cond in drains:
        copy = remote(size, size, ssem.at[at], l_sem.at[0], me, tp)
        if cond is None:
            copy.wait_send()
        else:
            pl.when(cond)(copy.wait_send)
    mark(None)


def mixer(d, args):
    G, near, far, rows, n_kv = d.groups, d.near, d.far, d.rows, d.n_kv
    dma = pltpu.SemaphoreType.DMA
    vmem, hbm = pl.BlockSpec(memory_space=pltpu.VMEM), pl.BlockSpec(memory_space=pltpu.HBM)

    def each(shape):
        return [pltpu.VMEM(shape(g), BF16) for g in range(G)]

    scratch = (
        each(lambda g: (near, d.depth, d.cols(g)))
        + each(lambda g: (near, d.depth, d.cols(g)))
        + each(lambda g: (far, near, rows, d.cols(g)))
        + each(lambda g: (far, near, rows, d.cols(g)))
        + each(lambda g: (near, rows, d.cols(g)))
        + each(lambda g: (near, rows, d.cols(g)))
        + each(lambda g: (d.gw, d.seqs * STATE_DIM))
        + each(lambda g: (n_kv, rows, d.gw))[: G - 1]
    )
    nb = d.feats // d.block
    hpad = -(-d.heads // LANES) * LANES
    per = n_kv // d.n_tp
    n_send = nb * d.n_tp + d.n_tp - 1 + 1 + 3 * G + G - 1 + 1 + 2 + 1 + 2 * (far - 1)
    n_local = G + 2 + len(args) - 6
    scratch = scratch + [
        pltpu.VMEM((nb, rows, d.block), BF16),
        pltpu.VMEM((near, far, rows, d.block), BF16),
        pltpu.VMEM((d.n_tp, rows, hpad + LANES), F32),
        pltpu.VMEM((d.n_tp, rows, hpad + LANES), F32),
        pltpu.VMEM((G * d.gw, d.out_cols), BF16),
        pltpu.VMEM((n_kv * rows, d.out_cols), F32),
        pltpu.VMEM((n_kv, rows, d.out_cols), BF16),
        pltpu.VMEM((n_kv, rows, d.out_cols), BF16),
        pltpu.VMEM((far, d.gw, d.out_cols), BF16),
        pltpu.VMEM((near, rows, d.gw), BF16),
        pltpu.VMEM((d.n_tp * near, per // near, rows, d.out_cols), BF16),
        pltpu.VMEM((d.n_tp * near, per // near, rows, d.out_cols), BF16),
        dma((n_send,)), dma((G,)), dma((far,)), dma((near, d.n_tp)), dma((d.n_tp,)),
        dma((G,)), dma((G,)), dma((max(G - 1, 1),)), dma((max(G - 1, 1),)), dma((1,)),
        dma((far,)), dma((1,)), dma((1,)), dma((n_local,)), dma((G,)),
    ]
    scratch = scratch + [pltpu.VMEM(item.shape, item.dtype) for item in args[6:]]
    past_v, past_b, past_c = (item.shape for item in args[-5:-2])
    return pl.pallas_call(
        functools.partial(mixer_kernel, d),
        out_shape=[
            pltpu.VMEM((d.seqs, d.props, d.feats), BF16),
            pltpu.VMEM((d.seqs, G * d.gw, STATE_DIM), F32),
            pltpu.VMEM(past_v, BF16),
            pltpu.VMEM(past_b, BF16),
            pltpu.VMEM(past_c, BF16),
            pltpu.VMEM((d.seqs, d.props, d.heads), BF16),
        ],
        in_specs=[hbm] * len(args),
        out_specs=[vmem] * 6,
        scratch_shapes=scratch,
        compiler_params=pltpu.CompilerParams(
            collective_id=0, has_side_effects=True, vmem_limit_bytes=24 * 2**20
        ),
        name="mixer",
    )(*(pltpu.with_memory_space_constraint(item, pltpu.HBM) for item in args))


def store_kernel(count, *refs):
    sem = refs[-1]
    copies = [
        pltpu.make_async_copy(refs[i], refs[count + i], sem.at[i]) for i in range(count)
    ]
    for copy in copies:
        copy.start()
    for copy in copies:
        copy.wait()


def store(items):
    count = len(items)
    return pl.pallas_call(
        functools.partial(store_kernel, count),
        out_shape=[jax.ShapeDtypeStruct(item.shape, item.dtype) for item in items],
        in_specs=[pl.BlockSpec(memory_space=pltpu.VMEM)] * count,
        out_specs=[pl.BlockSpec(memory_space=pltpu.HBM)] * count,
        scratch_shapes=[pltpu.SemaphoreType.DMA((count,))],
        compiler_params=pltpu.CompilerParams(vmem_limit_bytes=2**20),
        name="store",
    )(*items)


def on_device(
    tokens, input_gain, gate_weight, value_weight, write_weight, read_weight, step_weight,
    conv_value, conv_write, conv_read, step_bias, decay_log, skip_gain, output_gain, out_weight,
    base_state, past_value, past_write, past_read, past_step, accepted,
):
    seqs, props, feats = tokens.shape
    n_kv, n_tp = lax.axis_size("kv"), lax.axis_size("tp")
    depth, inner = gate_weight.shape
    groups = write_weight.shape[1] // STATE_DIM
    heads = step_bias.shape[0]
    gw = inner // groups
    near = near_size(n_kv, gw)
    d = Dims(
        far=n_kv // near, near=near, n_tp=n_tp, seqs=seqs, props=props,
        taps=conv_value.shape[0], width=feats * n_tp, feats=feats, depth=depth, groups=groups,
        gw=gw, heads=heads, out_cols=out_weight.shape[1],
    )

    def major(item):
        return item.transpose(1, 0, 2)

    def line(item):
        return item.reshape(1, item.shape[0])

    outs = mixer(
        d,
        (
            gate_weight, value_weight, write_weight, read_weight, out_weight,
            base_state.reshape(seqs, inner, STATE_DIM),
            tokens, line(input_gain), step_weight.T, conv_value, conv_write, conv_read,
            line(step_bias), line(decay_log), line(skip_gain), line(output_gain),
            major(past_value), major(past_write), major(past_read), past_step, line(accepted),
        ),
    )
    mixed, root, next_v, next_b, next_c, next_s = store(outs)
    return (
        mixed, root.reshape(base_state.shape), major(next_v), major(next_b), major(next_c), next_s,
    )


def solution(mesh):
    split = P("kv", None, "tp")
    weight = P("kv", "tp")
    state = P("kv", "tp", None, None)
    return jax.shard_map(
        on_device,
        mesh=mesh,
        in_specs=(
            split, P(), weight, weight, weight, weight, P(),
            P(None, "tp"), P(None, "tp"), P(None, "tp"),
            P("tp"), P("tp"), P("tp"), P("tp"),
            P("tp", "kv"),
            state, split, split, split, split, P("kv"),
        ),
        out_specs=(split, state, split, split, split, split),
        check_vma=False,
    )
```

```python
import functools
from typing import NamedTuple

import jax
import jax.numpy as jnp
from jax import lax
from jax.experimental import pallas as pl
from jax.experimental.pallas import tpu as pltpu
from jax.sharding import PartitionSpec as P

STATE_DIM = 128
LANES = 128
SMALL = 21
EPSILON = 1e-06
MESH = pl.DeviceIdType.MESH
F32 = jnp.float32
BF16 = jnp.bfloat16


class Dims(NamedTuple):
    far: int
    near: int
    n_tp: int
    seqs: int
    props: int
    taps: int
    width: int
    feats: int
    depth: int
    groups: int
    gw: int
    heads: int
    out_cols: int

    @property
    def rows(self):
        return self.seqs * self.props

    @property
    def n_kv(self):
        return self.far * self.near

    @property
    def block(self):
        return self.near * self.depth

    @property
    def part(self):
        return self.gw // self.near

    def thin(self, g):
        return g * self.near < 2 * self.groups

    def cols(self, g):
        return 2 * self.part + (STATE_DIM if self.thin(g) else 0)


def near_size(n_kv, gw):
    return max(
        d
        for d in range(2, n_kv + 1, 2)
        if n_kv % d == 0 and d * d <= n_kv and gw % (LANES * d) == 0
    )


def remote(src, dst, send, recv, kv, tp):
    return pltpu.make_async_remote_copy(
        src_ref=src,
        dst_ref=dst,
        send_sem=send,
        recv_sem=recv,
        device_id={"kv": kv, "tp": tp},
        device_id_type=MESH,
    )


def silu(v):
    return v / (1.0 + jnp.exp(-v))


def softplus(v):
    return jnp.maximum(v, 0.0) + jnp.log1p(jnp.exp(-jnp.abs(v)))


def conv(rows, taps, count):
    out = []
    for t in range(count):
        total = taps[0] * rows[t]
        for k in range(1, len(taps)):
            total = total + taps[k] * rows[t + k]
        out.append(total)
    return out


NT = (((1,), (1,)), ((), ()))


def mixer_kernel(d, *refs):
    gate_w, value_w, write_w, read_w, wout_h, base_h = refs[:6]
    small = refs[6:SMALL]
    mixed, base_v, next_v, next_b, next_c, next_s = refs[SMALL : SMALL + 6]
    rest = list(refs[SMALL + 6 :])
    G = d.groups
    stage, wbuf, zmine, zin, red, back, rootb = (rest[i * G : (i + 1) * G] for i in range(7))
    ys, rest = rest[7 * G : 8 * G - 1], rest[8 * G - 1 :]
    last = G - 1
    (
        xq, xs, pt_mine, pt_in, wout, acc, mine, parts, wlast, ylast, mine_l, parts_l,
        ssem, w_sem, xz_sem, xp_sem, pt_sem, z_sem, b_sem, yz_sem, yp_sem, m_sem,
        wl_sem, yl_sem, ml_sem, l_sem, g_sem,
    ) = rest[:27]
    held = rest[27:]
    (
        tok, gain, step_w, conv_v, conv_b, conv_c, bias_r, decay_r, skip_r, gain_out,
        past_v, past_b, past_c, past_s, taken_ref,
    ) = held
    far, near, n_tp, rows, S, N = d.far, d.near, d.n_tp, d.rows, d.seqs, STATE_DIM
    n_kv, part, gw, props = d.n_kv, d.part, d.gw, d.props
    me, tp = lax.axis_index("kv"), lax.axis_index("tp")
    h, l = lax.div(me, near), lax.rem(me, near)

    barrier = pltpu.get_barrier_semaphore()

    def greet(kv, t):
        pl.semaphore_signal(barrier, inc=1, device_id={"kv": kv, "tp": t}, device_id_type=MESH)

    for step in range(1, near):
        greet(h * near + lax.rem(l + step, near), tp)
    for t in range(n_tp):
        for step in range(1, far):
            greet(lax.rem(h + step, far) * near + l, t)
    for step in range(1, n_tp):
        greet(me, lax.rem(tp + step, n_tp))
    greeted = near - 1 + (far - 1) * n_tp + n_tp - 1

    class Mark:
        scope = None

        def __call__(self, name):
            if self.scope is not None:
                self.scope.__exit__(None, None, None)
            self.scope = None
            if name is not None:
                self.scope = jax.named_scope(name)
                self.scope.__enter__()

    mark = Mark()
    mark("prologue")
    used = []

    def local(src, dst):
        copy = pltpu.make_async_copy(src, dst, l_sem.at[len(used)])
        copy.start()
        used.append(copy)
        return copy

    fetch = [local(src, dst) for src, dst in zip(small, held)]
    units = 2 * G
    for g in range(G):
        def stage_in(src, dst):
            pltpu.make_async_copy(src, dst, g_sem.at[g]).start()

        for k in range(near):
            lo = g * gw + k * part
            stage_in(gate_w.at[:, lo : lo + part], stage[g].at[k, :, 0:part])
            stage_in(value_w.at[:, lo : lo + part], stage[g].at[k, :, part : 2 * part])
            if d.thin(g):
                u = (g * near + k) % units
                source = (write_w, read_w)[u % 2]
                stage_in(
                    source.at[:, u // 2 * N : (u // 2 + 1) * N],
                    stage[g].at[k, :, 2 * part : 2 * part + N],
                )
    loading = [
        local(base_h.at[:, g * gw : (g + 1) * gw], base_v.at[:, g * gw : (g + 1) * gw])
        for g in range(G)
    ]
    wlast_load = local(wout_h.at[last * gw : G * gw], wlast.at[h])
    wout_load = local(wout_h, wout)

    drains = []

    def meter(ref, count):
        at = len(drains)
        size = ref if count is None else ref.at[pl.ds(0, count)]
        drains.append((size, at, None))
        return at

    def alone(src, cond=None):
        drains.append((src, len(drains), cond))
        return len(drains) - 1

    def send(src, dst, recv, kv, t, cond=None, via=None):
        at = alone(src, cond) if via is None else via
        copy = remote(src, dst, ssem.at[at], recv, kv, t)
        if cond is None:
            copy.start()
        else:
            pl.when(cond)(copy.start)

    def arrive(dst, recv, cond=None):
        copy = remote(dst, dst, ssem.at[0], recv, me, tp)
        if cond is None:
            copy.wait_recv()
        else:
            pl.when(cond)(copy.wait_recv)

    def first(ref, count):
        return ref.at[pl.ds(0, count)]

    nb = d.feats // d.block
    own = pl.multiple_of(tp * d.feats, d.feats)
    for copy in fetch:
        copy.wait()
    order = lax.broadcasted_iota(jnp.int32, (rows, rows), 0)
    other = lax.broadcasted_iota(jnp.int32, (rows, rows), 1)

    def shuffle(major, minor):
        source = lax.rem(order, minor) * major + lax.div(order, minor)
        return jnp.where(other == source, 1.0, 0.0).astype(BF16)

    to_time, to_seq = shuffle(props, S), shuffle(S, props)

    def time_major(ref):
        stacked = jnp.concatenate([ref[s].astype(F32) for s in range(S)], axis=0).astype(BF16)
        return jnp.dot(to_time, stacked, preferred_element_type=F32)

    def put_seq(ref, cols, value):
        value = jnp.dot(to_seq, value, preferred_element_type=F32)
        for s in range(S):
            ref[s, :, cols] = value[s * props : (s + 1) * props].astype(BF16)

    raw = time_major(tok)
    square = jnp.sum(raw * raw, axis=-1, keepdims=True)
    scaled = (raw * gain[:, pl.ds(own, d.feats)]).astype(BF16)
    for q in range(nb):
        xq[q] = scaled[:, q * d.block : (q + 1) * d.block]
    hpad = pt_mine.shape[2] - LANES
    for t in range(n_tp):
        term = lax.dot_general(
            scaled, step_w[t * d.heads : (t + 1) * d.heads, pl.ds(own, d.feats)], NT,
            preferred_element_type=F32,
        )
        pt_mine[t, :, 0 : d.heads] = term
        pt_mine[t, :, hpad : hpad + LANES] = jnp.broadcast_to(square, (rows, LANES))
    pt_in[tp] = pt_mine[tp]

    mark('barrier')
    pl.semaphore_wait(barrier, greeted)

    mark('tok_send')
    home = lax.div(h, nb)
    for q in range(nb):
        plane = tp * nb + q
        for t in range(n_tp):
            away = jnp.logical_or(plane != h, tp != t)
            send(xq.at[q], xs.at[l, h], xz_sem.at[h], plane * near + l, t, away)

    @pl.when(home == tp)
    def _():
        xs[l, h] = xq[lax.rem(h, nb)]

    for step in range(1, n_tp):
        t = lax.rem(tp + step, n_tp)
        send(pt_mine.at[t], pt_in.at[tp], pt_sem.at[tp], me, t)

    def send_weights(g):
        arrive(stage[g], g_sem.at[g])
        via = meter(stage[g], near - 1)
        for step in range(1, near):
            k = lax.rem(l + step, near)
            send(stage[g].at[k], wbuf[g].at[l], w_sem.at[g], h * near + k, tp, via=via)

    send_weights(0)
    wlast_load.wait()

    def inside(z):
        return jnp.logical_and(z >= 0, z < far)

    def relay(level):
        for way in (1, -1):
            z = h - way * level
            block = lax.rem(z + far, far)
            if level:
                arrive(wlast.at[block], wl_sem.at[block], inside(z))
            if level < far - 1:
                peer = lax.rem(h + way + far, far) * near + l
                go = jnp.logical_and(inside(z), inside(h + way))
                send(wlast.at[block], wlast.at[block], wl_sem.at[block], peer, tp, go)

    diagonal = lax.broadcasted_iota(jnp.int32, (S, S), 0) == lax.broadcasted_iota(
        jnp.int32, (S, S), 1
    )
    taken = jnp.sum(
        jnp.where(diagonal, taken_ref[...].astype(F32), 0.0), axis=-1, keepdims=True
    ).astype(jnp.int32)
    steps_old = time_major(past_s).astype(BF16)
    head_rows = jnp.concatenate(
        [bias_r[...], decay_r[...], skip_r[...]] + [jnp.zeros_like(bias_r[...])] * 5, axis=0
    )
    params = []
    row_seq = lax.rem(lax.broadcasted_iota(jnp.int32, (rows, N), 0), S)

    def spread(g):
        r = lax.broadcasted_iota(jnp.int32, (d.heads, gw), 0)
        c = lax.broadcasted_iota(jnp.int32, (d.heads, gw), 1)
        hw = gw * G // d.heads
        lo = r * hw - g * gw
        return jnp.where(jnp.logical_and(c >= lo, c < lo + hw), 1.0, 0.0).astype(BF16)

    def span(g, w):
        return slice(g * w, (g + 1) * w)

    def taps(ref, cols):
        return [ref[k : k + 1, cols] for k in range(d.taps)]

    def param(k, g):
        if g == len(params):
            params.append(
                jnp.dot(
                    head_rows, spread(g).astype(F32), preferred_element_type=F32,
                    precision=lax.Precision.HIGHEST,
                )
            )
        return params[g][k : k + 1]

    def pieces(v):
        return [v[t * S : (t + 1) * S] for t in range(props)]

    def old(ref, cols):
        return [ref[i, :, cols].astype(F32) for i in range(ref.shape[0])]

    def root(g):
        mark(f'root{g}')
        loading[g].wait()
        cv, cn = span(g, gw), span(g, N)
        px = [silu(v) for v in conv(old(past_v, cv), taps(conv_v, cv), props)]
        pb = [silu(v) for v in conv(old(past_b, cn), taps(conv_b, cn), props)]
        pd = softplus(
            jnp.dot(steps_old, spread(g), preferred_element_type=F32) + param(0, g)
        )
        rate = jnp.exp(param(1, g))
        pd = pieces(pd)
        log = [jnp.where(taken > t, -rate * pd[t], 0.0) for t in range(props)]
        tail = jnp.zeros_like(log[0])
        weighted = [None] * props
        for t in reversed(range(props)):
            weighted[t] = jnp.where(taken > t, jnp.exp(tail) * pd[t], 0.0) * px[t]
            tail = tail + log[t]
        left = jnp.transpose(jnp.concatenate(weighted, axis=0)).astype(BF16)
        decay = jnp.exp(tail)
        fill = [decay] * max(1, 8 // S)
        decay = jnp.transpose(jnp.concatenate(fill, axis=0))
        right = jnp.concatenate(pb, axis=0)
        for s in range(S):
            outer = jnp.dot(
                left,
                jnp.where(row_seq == s, right, 0.0).astype(BF16),
                preferred_element_type=F32,
            )
            new = decay[:, s : s + 1] * base_v[s, cv, :] + outer
            base_v[s, cv, :] = new
            rootb[g][:, span(s, N)] = new.astype(BF16)

    for g in range(max(1, G - 1)):
        root(g)

    mark('tokz_wait')
    for k in range(far):
        arrive(
            xs.at[l, k], xz_sem.at[k], jnp.logical_or(h != k, home != tp)
        )
    fq = far // n_tp

    def piece(k, t):
        return xs.at[k, pl.ds(t * fq, fq)]

    via_x = meter(xs, near - 1)
    for step in range(1, near):
        k = h * near + lax.rem(l + step, near)
        send(piece(l, tp), piece(l, tp), xp_sem.at[l, tp], k, tp, via=via_x)
    for g in range(1, G):
        send_weights(g)
    relay(0)
    if G > 1:
        root(G - 1)

    mark('scale')
    for step in range(1, n_tp):
        t = lax.rem(tp + n_tp - step, n_tp)
        arrive(pt_in.at[t], pt_sem.at[t])
    joined = pt_in[0]
    for t in range(1, n_tp):
        joined = joined + pt_in[t]
    scale = lax.rsqrt(joined[:, hpad : hpad + LANES] * (1.0 / d.width) + EPSILON)
    step_now = (joined[:, 0 : d.heads] * scale[:, 0 : d.heads]).astype(BF16)
    put_seq(next_s, slice(None), step_now)

    def weights(g):
        mark(f'w_wait{g}')
        wbuf[g][l] = stage[g][l]
        arrive(first(wbuf[g], near - 1), w_sem.at[g])
        mark(f'matmul{g}')
        return wbuf[g][...].reshape(d.block, d.cols(g))

    def product(g, left, weight):
        return jnp.dot(left, weight, preferred_element_type=F32).astype(BF16)

    via_z = {}

    def early():
        result = product(0, xs[l].reshape(far * rows, d.block), weights(0))
        for z in range(far):
            zmine[0][z, l] = result[z * rows : (z + 1) * rows]
        via_z[0] = meter(zmine[0], far - 1)
        for step in reversed(range(1, far)):
            z = lax.rem(h + step, far)
            src, dst = zmine[0].at[z, l], zin[0].at[h, l]
            send(src, dst, z_sem.at[0], z * near + l, tp, via=via_z[0])

    def project(g):
        if g == 0:
            mark('matmul0b')
            places = [lax.rem(l + step, near) for step in range(1, near)]
            left = jnp.concatenate(
                [xs[k].reshape(far * rows, d.block) for k in places], axis=0
            )
            result = product(0, left, wbuf[0][...].reshape(d.block, d.cols(0)))
            for i, k in enumerate(places):
                for z in range(far):
                    at = (i * far + z) * rows
                    zmine[0][z, k] = result[at : at + rows]
            for step in reversed(range(1, far)):
                z = lax.rem(h + step, far)
                for k in places:
                    src, dst = zmine[0].at[z, k], zin[0].at[h, k]
                    send(src, dst, z_sem.at[0], z * near + l, tp, via=via_z[0])
            return
        result = product(g, xs[...].reshape(n_kv * rows, d.block), weights(g))
        for k in range(near):
            for z in range(far):
                at = (k * far + z) * rows
                zmine[g][z, k] = result[at : at + rows]
        via = meter(zmine[g], far - 1)
        for step in reversed(range(1, far)):
            z = lax.rem(h + step, far)
            send(zmine[g].at[z], zin[g].at[h], z_sem.at[g], z * near + l, tp, via=via)

    early()
    mark('tokp_wait')
    for step in range(1, near):
        k = lax.rem(l + near - step, near)
        arrive(piece(k, tp), xp_sem.at[k, tp])
        for side in range(1, n_tp):
            t = lax.rem(tp + side, n_tp)
            send(piece(k, tp), piece(k, tp), xp_sem.at[k, tp], me, t, via=via_x)
    for step in range(1, near):
        k = lax.rem(l + near - step, near)
        for side in range(1, n_tp):
            t = lax.rem(tp + n_tp - side, n_tp)
            arrive(piece(k, t), xp_sem.at[k, t])

    def collect(g):
        mark(f'z_wait{g}')
        arrive(first(zin[g], far - 1), z_sem.at[g])
        value = zmine[g][h].astype(F32)
        for step in range(1, far):
            z = lax.rem(h + far - step, far)
            value = value + zin[g][z].astype(F32)
        red[g][...] = value.astype(BF16)
        back[g][l] = red[g][l]
        via = meter(red[g], near - 1)
        for step in range(1, near):
            k = lax.rem(l + step, near)
            send(red[g].at[k], back[g].at[l], b_sem.at[g], h * near + k, tp, via=via)

    def rounded(piece):
        return (piece.astype(F32) * scale).astype(BF16).astype(F32)

    via_y = {}

    def advance(g):
        mark(f'b_wait{g}')
        arrive(first(back[g], near - 1), b_sem.at[g])
        cv, cn = span(g, gw), span(g, N)
        mark(f'advance{g}')
        gate = jnp.concatenate([rounded(back[g][k, :, 0:part]) for k in range(near)], axis=1)
        value = jnp.concatenate(
            [rounded(back[g][k, :, part : 2 * part]) for k in range(near)], axis=1
        )

        def unit(u):
            j, k = u // near, u % near
            return rounded(back[j][k, :, 2 * part : 2 * part + N])

        def window(past, now, out, cols):
            before = old(past, cols)
            rows_now = []
            for i in range(d.taps - 1):
                row = before[i + 1]
                for a in range(2, props + 1):
                    row = jnp.where(taken == a, before[i + a], row)
                rows_now.append(row)
            rows_now = rows_now + pieces(now)
            for i, row in enumerate(rows_now):
                out[i, :, cols] = row.astype(BF16)
            return rows_now

        win_v = window(past_v, value, next_v, cv)
        win_b = window(past_b, unit(2 * g), next_b, cn)
        win_c = window(past_c, unit(2 * g + 1), next_c, cn)
        x = [silu(v) for v in conv(win_v, taps(conv_v, cv), props)]
        b = [silu(v) for v in conv(win_b, taps(conv_b, cn), props)]
        c = [silu(v) for v in conv(win_c, taps(conv_c, cn), props)]
        whole = jnp.concatenate(c, axis=0)
        masked = jnp.concatenate(
            [jnp.where(row_seq == s, whole, 0.0) for s in range(S)], axis=1
        ).astype(BF16)
        carried = pieces(
            lax.dot_general(masked, rootb[g][...], NT, preferred_element_type=F32)
        )
        dt = pieces(
            softplus(jnp.dot(step_now, spread(g), preferred_element_type=F32) + param(0, g))
        )
        rate = jnp.exp(param(1, g))
        logs = []
        for t in range(props):
            log = -rate * dt[t]
            logs.append(log if t == 0 else logs[-1] + log)
        y = []
        for t in range(props):
            row = jnp.exp(logs[t]) * carried[t] + param(2, g) * x[t]
            for s in range(t + 1):
                score = jnp.sum(c[t] * b[s], axis=-1, keepdims=True)
                weight = dt[s] if s == t else jnp.exp(logs[t] - logs[s]) * dt[s]
                row = row + (score * weight) * x[s]
            y.append(row)
        gated = jnp.concatenate(y, axis=0) * silu(gate)
        mean = jnp.sum(gated * gated, axis=-1, keepdims=True) * (1.0 / gw)
        normal = (gated * lax.rsqrt(mean + EPSILON) * gain_out[:, cv]).astype(BF16)
        if g == last:
            ylast[l] = normal
            via = meter(ylast, near - 1)
            for step in range(1, near):
                k = lax.rem(l + step, near)
                send(ylast.at[l], ylast.at[l], yl_sem.at[0], h * near + k, tp, via=via)
            return
        ys[g][me] = normal
        via_y[g] = meter(ys[g], n_kv - 1)
        for step in reversed(range(1, far)):
            z = lax.rem(h + step, far)
            spot = ys[g].at[me]
            send(spot, spot, yz_sem.at[g], z * near + l, tp, via=via_y[g])
        for step in range(1, near):
            k = lax.rem(l + step, near)
            send(spot, spot, yp_sem.at[g], h * near + k, tp, via=via_y[g])

    def forward(g):
        mark(f'yz_wait{g}')
        arrive(first(ys[g], far - 1), yz_sem.at[g])
        for step in range(1, far):
            spot = ys[g].at[lax.rem(h + far - step, far) * near + l]
            for side in range(1, near):
                k = lax.rem(l + side, near)
                send(spot, spot, yp_sem.at[g], h * near + k, tp, via=via_y[g])

    def output(g):
        mark(f'y_wait{g}')
        arrive(first(ys[g], (near - 1) * far), yp_sem.at[g])
        if g == 0:
            wout_load.wait()
        mark(f'out{g}')
        term = jnp.dot(
            ys[g][...].reshape(n_kv * rows, gw), wout[span(g, gw), :], preferred_element_type=F32
        )
        if g == 0:
            acc[...] = term
        else:
            acc[...] += term

    cols = d.out_cols
    per = n_kv // n_tp
    side, place = lax.div(me, per), lax.rem(me, per)
    deep = per // near

    def share():
        mark('share')
        mine[...] = acc[...].astype(BF16).reshape(n_kv, rows, cols)
        via = meter(mine, n_kv - 1)
        slot = parts.at[tp * per + place]
        for step in range(1, n_kv):
            k = lax.rem(me + step, n_kv)
            send(mine.at[k], slot, m_sem.at[0], k, side, via=via)
        send(mine.at[me], slot, m_sem.at[0], me, side, side != tp)

        @pl.when(side == tp)
        def _():
            parts[tp * per + place] = mine[me]

    def output_last():
        mark('wl_wait')
        for level in levels:
            relay(level)
        if not last:
            wout_load.wait()
        mark('yl_wait')
        arrive(first(ylast, near - 1), yl_sem.at[0])
        mark('outl')
        every = ylast[...].reshape(near * rows, gw)
        for z in range(far):
            term = jnp.dot(every, wlast[z], preferred_element_type=F32).astype(BF16)
            for k in range(near):
                mine_l[z // deep * near + k, z % deep] = term[k * rows : (k + 1) * rows]
        via = meter(mine_l, near * n_tp - 1)
        spot = tp * near + l
        for step in range(1, near * n_tp):
            to = lax.rem(spot + step, near * n_tp)
            send(
                mine_l.at[to], parts_l.at[spot], ml_sem.at[0],
                h * near + lax.rem(to, near), lax.div(to, near), via=via,
            )
        parts_l[spot] = mine_l[spot]

    plan = (
        (project, lambda g: 2.75 * g),
        (collect, lambda g: 8.0 + 3.0 * g if g else 5.6),
        (advance, lambda g: 12.0 + 2.7 * g if g else 9.0),
        (forward, lambda g: 17.6 + 1.9 * g),
    )
    order_of = sorted(
        (when(g), i, g)
        for i, (_, when) in enumerate(plan)
        for g in range(G if i < 3 else last)
    )
    levels = iter(range(1, far))
    for _, i, g in order_of:
        plan[i][0](g)
        if far > 3 and g == last - 1 and i > 1:
            relay(next(levels))

    for g in range(last):
        output(g)
    if last:
        share()
    output_last()

    mark('final_wait')
    if last:
        arrive(first(parts, n_kv - 1), m_sem.at[0], side == tp)
        arrive(parts, m_sem.at[0], side != tp)
    mark('final_last')
    arrive(first(parts_l, near * n_tp - 1), ml_sem.at[0])
    for k in range(per):
        value = None
        for t in range(n_tp):
            terms = [parts_l[t * near + k % near, k // near]]
            terms = terms + ([parts[t * per + k]] if last else [])
            for term in terms:
                term = term.astype(F32)
                value = term if value is None else value + term
        put_seq(mixed, span(k, cols), value.astype(BF16))
    mark('drain')
    for size, at, cond in drains:
        copy = remote(size, size, ssem.at[at], l_sem.at[0], me, tp)
        if cond is None:
            copy.wait_send()
        else:
            pl.when(cond)(copy.wait_send)
    mark(None)


def mixer(d, args):
    G, near, far, rows, n_kv = d.groups, d.near, d.far, d.rows, d.n_kv
    dma = pltpu.SemaphoreType.DMA
    vmem, hbm = pl.BlockSpec(memory_space=pltpu.VMEM), pl.BlockSpec(memory_space=pltpu.HBM)

    def each(shape):
        return [pltpu.VMEM(shape(g), BF16) for g in range(G)]

    scratch = (
        each(lambda g: (near, d.depth, d.cols(g)))
        + each(lambda g: (near, d.depth, d.cols(g)))
        + each(lambda g: (far, near, rows, d.cols(g)))
        + each(lambda g: (far, near, rows, d.cols(g)))
        + each(lambda g: (near, rows, d.cols(g)))
        + each(lambda g: (near, rows, d.cols(g)))
        + each(lambda g: (d.gw, d.seqs * STATE_DIM))
        + each(lambda g: (n_kv, rows, d.gw))[: G - 1]
    )
    nb = d.feats // d.block
    hpad = -(-d.heads // LANES) * LANES
    per = n_kv // d.n_tp
    n_send = nb * d.n_tp + d.n_tp - 1 + 1 + 3 * G + G - 1 + 1 + 2 + 1 + 2 * (far - 1)
    n_local = G + 2 + len(args) - 6
    scratch = scratch + [
        pltpu.VMEM((nb, rows, d.block), BF16),
        pltpu.VMEM((near, far, rows, d.block), BF16),
        pltpu.VMEM((d.n_tp, rows, hpad + LANES), F32),
        pltpu.VMEM((d.n_tp, rows, hpad + LANES), F32),
        pltpu.VMEM((G * d.gw, d.out_cols), BF16),
        pltpu.VMEM((n_kv * rows, d.out_cols), F32),
        pltpu.VMEM((n_kv, rows, d.out_cols), BF16),
        pltpu.VMEM((n_kv, rows, d.out_cols), BF16),
        pltpu.VMEM((far, d.gw, d.out_cols), BF16),
        pltpu.VMEM((near, rows, d.gw), BF16),
        pltpu.VMEM((d.n_tp * near, per // near, rows, d.out_cols), BF16),
        pltpu.VMEM((d.n_tp * near, per // near, rows, d.out_cols), BF16),
        dma((n_send,)), dma((G,)), dma((far,)), dma((near, d.n_tp)), dma((d.n_tp,)),
        dma((G,)), dma((G,)), dma((max(G - 1, 1),)), dma((max(G - 1, 1),)), dma((1,)),
        dma((far,)), dma((1,)), dma((1,)), dma((n_local,)), dma((G,)),
    ]
    scratch = scratch + [pltpu.VMEM(item.shape, item.dtype) for item in args[6:]]
    past_v, past_b, past_c = (item.shape for item in args[-5:-2])
    return pl.pallas_call(
        functools.partial(mixer_kernel, d),
        out_shape=[
            pltpu.VMEM((d.seqs, d.props, d.feats), BF16),
            pltpu.VMEM((d.seqs, G * d.gw, STATE_DIM), F32),
            pltpu.VMEM(past_v, BF16),
            pltpu.VMEM(past_b, BF16),
            pltpu.VMEM(past_c, BF16),
            pltpu.VMEM((d.seqs, d.props, d.heads), BF16),
        ],
        in_specs=[hbm] * len(args),
        out_specs=[vmem] * 6,
        scratch_shapes=scratch,
        compiler_params=pltpu.CompilerParams(
            collective_id=0, has_side_effects=True, vmem_limit_bytes=24 * 2**20
        ),
        name="mixer",
    )(*(pltpu.with_memory_space_constraint(item, pltpu.HBM) for item in args))


def store_kernel(count, *refs):
    sem = refs[-1]
    copies = [
        pltpu.make_async_copy(refs[i], refs[count + i], sem.at[i]) for i in range(count)
    ]
    for copy in copies:
        copy.start()
    for copy in copies:
        copy.wait()


def store(items):
    count = len(items)
    return pl.pallas_call(
        functools.partial(store_kernel, count),
        out_shape=[jax.ShapeDtypeStruct(item.shape, item.dtype) for item in items],
        in_specs=[pl.BlockSpec(memory_space=pltpu.VMEM)] * count,
        out_specs=[pl.BlockSpec(memory_space=pltpu.HBM)] * count,
        scratch_shapes=[pltpu.SemaphoreType.DMA((count,))],
        compiler_params=pltpu.CompilerParams(vmem_limit_bytes=2**20),
        name="store",
    )(*items)


def on_device(
    tokens, input_gain, gate_weight, value_weight, write_weight, read_weight, step_weight,
    conv_value, conv_write, conv_read, step_bias, decay_log, skip_gain, output_gain, out_weight,
    base_state, past_value, past_write, past_read, past_step, accepted,
):
    seqs, props, feats = tokens.shape
    n_kv, n_tp = lax.axis_size("kv"), lax.axis_size("tp")
    depth, inner = gate_weight.shape
    groups = write_weight.shape[1] // STATE_DIM
    heads = step_bias.shape[0]
    gw = inner // groups
    near = near_size(n_kv, gw)
    d = Dims(
        far=n_kv // near, near=near, n_tp=n_tp, seqs=seqs, props=props,
        taps=conv_value.shape[0], width=feats * n_tp, feats=feats, depth=depth, groups=groups,
        gw=gw, heads=heads, out_cols=out_weight.shape[1],
    )

    def major(item):
        return item.transpose(1, 0, 2)

    def line(item):
        return item.reshape(1, item.shape[0])

    outs = mixer(
        d,
        (
            gate_weight, value_weight, write_weight, read_weight, out_weight,
            base_state.reshape(seqs, inner, STATE_DIM),
            tokens, line(input_gain), step_weight.T, conv_value, conv_write, conv_read,
            line(step_bias), line(decay_log), line(skip_gain), line(output_gain),
            major(past_value), major(past_write), major(past_read), past_step, line(accepted),
        ),
    )
    mixed, root, next_v, next_b, next_c, next_s = store(outs)
    return (
        mixed, root.reshape(base_state.shape), major(next_v), major(next_b), major(next_c), next_s,
    )


def solution(mesh):
    split = P("kv", None, "tp")
    weight = P("kv", "tp")
    state = P("kv", "tp", None, None)
    return jax.shard_map(
        on_device,
        mesh=mesh,
        in_specs=(
            split, P(), weight, weight, weight, weight, P(),
            P(None, "tp"), P(None, "tp"), P(None, "tp"),
            P("tp"), P("tp"), P("tp"), P("tp"),
            P("tp", "kv"),
            state, split, split, split, split, P("kv"),
        ),
        out_specs=(split, state, split, split, split, split),
        check_vma=False,
    )
```

```python
import functools
from typing import NamedTuple

import jax
import jax.numpy as jnp
from jax import lax
from jax.experimental import pallas as pl
from jax.experimental.pallas import tpu as pltpu
from jax.sharding import PartitionSpec as P

STATE_DIM = 128
LANES = 128
SMALL = 21
EPSILON = 1e-06
MESH = pl.DeviceIdType.MESH
F32 = jnp.float32
BF16 = jnp.bfloat16


class Dims(NamedTuple):
    far: int
    near: int
    n_tp: int
    seqs: int
    props: int
    taps: int
    width: int
    feats: int
    depth: int
    groups: int
    gw: int
    heads: int
    out_cols: int

    @property
    def rows(self):
        return self.seqs * self.props

    @property
    def n_kv(self):
        return self.far * self.near

    @property
    def block(self):
        return self.near * self.depth

    @property
    def part(self):
        return self.gw // self.near

    def thin(self, g):
        return 2 * g % self.near == 0

    def cols(self, g):
        return 2 * self.part + (STATE_DIM if self.thin(g) else 0)


def near_size(n_kv, gw):
    return max(
        d
        for d in range(2, n_kv + 1, 2)
        if n_kv % d == 0 and d * d <= n_kv and gw % (LANES * d) == 0
    )


def remote(src, dst, send, recv, kv, tp):
    return pltpu.make_async_remote_copy(
        src_ref=src,
        dst_ref=dst,
        send_sem=send,
        recv_sem=recv,
        device_id={"kv": kv, "tp": tp},
        device_id_type=MESH,
    )


def silu(v):
    return v / (1.0 + jnp.exp(-v))


def softplus(v):
    return jnp.maximum(v, 0.0) + jnp.log1p(jnp.exp(-jnp.abs(v)))


def conv(rows, taps, count):
    out = []
    for t in range(count):
        total = taps[0] * rows[t]
        for k in range(1, len(taps)):
            total = total + taps[k] * rows[t + k]
        out.append(total)
    return out


NT = (((1,), (1,)), ((), ()))


def mixer_kernel(d, *refs):
    gate_w, value_w, write_w, read_w, wout_h, base_h = refs[:6]
    small = refs[6:SMALL]
    mixed, base_v, next_v, next_b, next_c, next_s = refs[SMALL : SMALL + 6]
    rest = list(refs[SMALL + 6 :])
    G = d.groups
    stage, wbuf, zmine, zin, red, back, rootb = (rest[i * G : (i + 1) * G] for i in range(7))
    ys, rest = rest[7 * G : 8 * G - 1], rest[8 * G - 1 :]
    last = G - 1
    (
        xq, xs, pt_mine, pt_in, wout, acc, mine, parts, wlast, ylast, mine_l, parts_l,
        ssem, w_sem, xz_sem, xp_sem, pt_sem, z_sem, b_sem, yz_sem, yp_sem, m_sem,
        wl_sem, yl_sem, ml_sem, l_sem, g_sem,
    ) = rest[:27]
    held = rest[27:]
    (
        tok, gain, step_w, conv_v, conv_b, conv_c, bias_r, decay_r, skip_r, gain_out,
        past_v, past_b, past_c, past_s, taken_ref,
    ) = held
    far, near, n_tp, rows, S, N = d.far, d.near, d.n_tp, d.rows, d.seqs, STATE_DIM
    n_kv, part, gw, props = d.n_kv, d.part, d.gw, d.props
    me, tp = lax.axis_index("kv"), lax.axis_index("tp")
    h, l = lax.div(me, near), lax.rem(me, near)

    barrier = pltpu.get_barrier_semaphore()

    def greet(kv, t):
        pl.semaphore_signal(barrier, inc=1, device_id={"kv": kv, "tp": t}, device_id_type=MESH)

    for step in range(1, near):
        greet(h * near + lax.rem(l + step, near), tp)
    for t in range(n_tp):
        for step in range(1, far):
            greet(lax.rem(h + step, far) * near + l, t)
    for step in range(1, n_tp):
        greet(me, lax.rem(tp + step, n_tp))
    greeted = near - 1 + (far - 1) * n_tp + n_tp - 1

    class Mark:
        scope = None

        def __call__(self, name):
            if self.scope is not None:
                self.scope.__exit__(None, None, None)
            self.scope = None
            if name is not None:
                self.scope = jax.named_scope(name)
                self.scope.__enter__()

    mark = Mark()
    mark("prologue")
    used = []

    def local(src, dst):
        copy = pltpu.make_async_copy(src, dst, l_sem.at[len(used)])
        copy.start()
        used.append(copy)
        return copy

    fetch = [local(src, dst) for src, dst in zip(small, held)]
    units = 2 * G
    for g in range(G):
        def stage_in(src, dst):
            pltpu.make_async_copy(src, dst, g_sem.at[g]).start()

        for k in range(near):
            lo = g * gw + k * part
            stage_in(gate_w.at[:, lo : lo + part], stage[g].at[k, :, 0:part])
            stage_in(value_w.at[:, lo : lo + part], stage[g].at[k, :, part : 2 * part])
            if d.thin(g):
                u = (2 * g + k) % units
                source = (write_w, read_w)[u % 2]
                stage_in(
                    source.at[:, u // 2 * N : (u // 2 + 1) * N],
                    stage[g].at[k, :, 2 * part : 2 * part + N],
                )
    loading = [
        local(base_h.at[:, g * gw : (g + 1) * gw], base_v.at[:, g * gw : (g + 1) * gw])
        for g in range(G)
    ]
    wlast_load = local(wout_h.at[last * gw : G * gw], wlast.at[h])
    wout_load = local(wout_h, wout)

    drains = []

    def meter(ref, count):
        at = len(drains)
        size = ref if count is None else ref.at[pl.ds(0, count)]
        drains.append((size, at, None))
        return at

    def alone(src, cond=None):
        drains.append((src, len(drains), cond))
        return len(drains) - 1

    def send(src, dst, recv, kv, t, cond=None, via=None):
        at = alone(src, cond) if via is None else via
        copy = remote(src, dst, ssem.at[at], recv, kv, t)
        if cond is None:
            copy.start()
        else:
            pl.when(cond)(copy.start)

    def arrive(dst, recv, cond=None):
        copy = remote(dst, dst, ssem.at[0], recv, me, tp)
        if cond is None:
            copy.wait_recv()
        else:
            pl.when(cond)(copy.wait_recv)

    def first(ref, count):
        return ref.at[pl.ds(0, count)]

    nb = d.feats // d.block
    own = pl.multiple_of(tp * d.feats, d.feats)
    for copy in fetch:
        copy.wait()
    order = lax.broadcasted_iota(jnp.int32, (rows, rows), 0)
    other = lax.broadcasted_iota(jnp.int32, (rows, rows), 1)

    def shuffle(major, minor):
        source = lax.rem(order, minor) * major + lax.div(order, minor)
        return jnp.where(other == source, 1.0, 0.0).astype(BF16)

    to_time, to_seq = shuffle(props, S), shuffle(S, props)

    def time_major(ref):
        stacked = jnp.concatenate([ref[s].astype(F32) for s in range(S)], axis=0).astype(BF16)
        return jnp.dot(to_time, stacked, preferred_element_type=F32)

    def put_seq(ref, cols, value):
        value = jnp.dot(to_seq, value, preferred_element_type=F32)
        for s in range(S):
            ref[s, :, cols] = value[s * props : (s + 1) * props].astype(BF16)

    raw = time_major(tok)
    square = jnp.sum(raw * raw, axis=-1, keepdims=True)
    scaled = (raw * gain[:, pl.ds(own, d.feats)]).astype(BF16)
    for q in range(nb):
        xq[q] = scaled[:, q * d.block : (q + 1) * d.block]
    hpad = pt_mine.shape[2] - LANES
    for t in range(n_tp):
        term = lax.dot_general(
            scaled, step_w[t * d.heads : (t + 1) * d.heads, pl.ds(own, d.feats)], NT,
            preferred_element_type=F32,
        )
        pt_mine[t, :, 0 : d.heads] = term
        pt_mine[t, :, hpad : hpad + LANES] = jnp.broadcast_to(square, (rows, LANES))
    pt_in[tp] = pt_mine[tp]

    mark('barrier')
    pl.semaphore_wait(barrier, greeted)

    mark('tok_send')
    home = lax.div(h, nb)
    for q in range(nb):
        plane = tp * nb + q
        for t in range(n_tp):
            away = jnp.logical_or(plane != h, tp != t)
            send(xq.at[q], xs.at[l, h], xz_sem.at[h], plane * near + l, t, away)

    @pl.when(home == tp)
    def _():
        xs[l, h] = xq[lax.rem(h, nb)]

    for step in range(1, n_tp):
        t = lax.rem(tp + step, n_tp)
        send(pt_mine.at[t], pt_in.at[tp], pt_sem.at[tp], me, t)

    def send_weights(g):
        arrive(stage[g], g_sem.at[g])
        via = meter(stage[g], near - 1)
        for step in range(1, near):
            k = lax.rem(l + step, near)
            send(stage[g].at[k], wbuf[g].at[l], w_sem.at[g], h * near + k, tp, via=via)

    send_weights(0)
    wlast_load.wait()

    def inside(z):
        return jnp.logical_and(z >= 0, z < far)

    def relay(level):
        for way in (1, -1):
            z = h - way * level
            block = lax.rem(z + far, far)
            if level:
                arrive(wlast.at[block], wl_sem.at[block], inside(z))
            if level < far - 1:
                peer = lax.rem(h + way + far, far) * near + l
                go = jnp.logical_and(inside(z), inside(h + way))
                send(wlast.at[block], wlast.at[block], wl_sem.at[block], peer, tp, go)

    diagonal = lax.broadcasted_iota(jnp.int32, (S, S), 0) == lax.broadcasted_iota(
        jnp.int32, (S, S), 1
    )
    taken = jnp.sum(
        jnp.where(diagonal, taken_ref[...].astype(F32), 0.0), axis=-1, keepdims=True
    ).astype(jnp.int32)
    steps_old = time_major(past_s).astype(BF16)
    head_rows = jnp.concatenate(
        [bias_r[...], decay_r[...], skip_r[...]] + [jnp.zeros_like(bias_r[...])] * 5, axis=0
    )
    params = []
    row_seq = lax.rem(lax.broadcasted_iota(jnp.int32, (rows, N), 0), S)

    def spread(g):
        r = lax.broadcasted_iota(jnp.int32, (d.heads, gw), 0)
        c = lax.broadcasted_iota(jnp.int32, (d.heads, gw), 1)
        hw = gw * G // d.heads
        lo = r * hw - g * gw
        return jnp.where(jnp.logical_and(c >= lo, c < lo + hw), 1.0, 0.0).astype(BF16)

    def span(g, w):
        return slice(g * w, (g + 1) * w)

    def taps(ref, cols):
        return [ref[k : k + 1, cols] for k in range(d.taps)]

    def param(k, g):
        if g == len(params):
            params.append(
                jnp.dot(
                    head_rows, spread(g).astype(F32), preferred_element_type=F32,
                    precision=lax.Precision.HIGHEST,
                )
            )
        return params[g][k : k + 1]

    def pieces(v):
        return [v[t * S : (t + 1) * S] for t in range(props)]

    def old(ref, cols):
        return [ref[i, :, cols].astype(F32) for i in range(ref.shape[0])]

    def root(g):
        mark(f'root{g}')
        loading[g].wait()
        cv, cn = span(g, gw), span(g, N)
        px = [silu(v) for v in conv(old(past_v, cv), taps(conv_v, cv), props)]
        pb = [silu(v) for v in conv(old(past_b, cn), taps(conv_b, cn), props)]
        pd = softplus(
            jnp.dot(steps_old, spread(g), preferred_element_type=F32) + param(0, g)
        )
        rate = jnp.exp(param(1, g))
        pd = pieces(pd)
        log = [jnp.where(taken > t, -rate * pd[t], 0.0) for t in range(props)]
        tail = jnp.zeros_like(log[0])
        weighted = [None] * props
        for t in reversed(range(props)):
            weighted[t] = jnp.where(taken > t, jnp.exp(tail) * pd[t], 0.0) * px[t]
            tail = tail + log[t]
        left = jnp.transpose(jnp.concatenate(weighted, axis=0)).astype(BF16)
        decay = jnp.exp(tail)
        fill = [decay] * max(1, 8 // S)
        decay = jnp.transpose(jnp.concatenate(fill, axis=0))
        right = jnp.concatenate(pb, axis=0)
        for s in range(S):
            outer = jnp.dot(
                left,
                jnp.where(row_seq == s, right, 0.0).astype(BF16),
                preferred_element_type=F32,
            )
            new = decay[:, s : s + 1] * base_v[s, cv, :] + outer
            base_v[s, cv, :] = new
            rootb[g][:, span(s, N)] = new.astype(BF16)

    for g in range(max(1, G - 1)):
        root(g)

    mark('tokz_wait')
    for k in range(far):
        arrive(
            xs.at[l, k], xz_sem.at[k], jnp.logical_or(h != k, home != tp)
        )
    fq = far // n_tp

    def piece(k, t):
        return xs.at[k, pl.ds(t * fq, fq)]

    via_x = meter(xs, near - 1)
    for step in range(1, near):
        k = h * near + lax.rem(l + step, near)
        send(piece(l, tp), piece(l, tp), xp_sem.at[l, tp], k, tp, via=via_x)
    for g in range(1, G):
        send_weights(g)
    relay(0)
    if G > 1:
        root(G - 1)

    mark('scale')
    for step in range(1, n_tp):
        t = lax.rem(tp + n_tp - step, n_tp)
        arrive(pt_in.at[t], pt_sem.at[t])
    joined = pt_in[0]
    for t in range(1, n_tp):
        joined = joined + pt_in[t]
    scale = lax.rsqrt(joined[:, hpad : hpad + LANES] * (1.0 / d.width) + EPSILON)
    step_now = (joined[:, 0 : d.heads] * scale[:, 0 : d.heads]).astype(BF16)
    put_seq(next_s, slice(None), step_now)

    def weights(g):
        mark(f'w_wait{g}')
        wbuf[g][l] = stage[g][l]
        arrive(first(wbuf[g], near - 1), w_sem.at[g])
        mark(f'matmul{g}')
        return wbuf[g][...].reshape(d.block, d.cols(g))

    def product(g, left, weight):
        return jnp.dot(left, weight, preferred_element_type=F32).astype(BF16)

    via_z = {}

    def early():
        result = product(0, xs[l].reshape(far * rows, d.block), weights(0))
        for z in range(far):
            zmine[0][z, l] = result[z * rows : (z + 1) * rows]
        via_z[0] = meter(zmine[0], far - 1)
        for step in reversed(range(1, far)):
            z = lax.rem(h + step, far)
            src, dst = zmine[0].at[z, l], zin[0].at[h, l]
            send(src, dst, z_sem.at[0], z * near + l, tp, via=via_z[0])

    def project(g):
        if g == 0:
            mark('matmul0b')
            places = [lax.rem(l + step, near) for step in range(1, near)]
            left = jnp.concatenate(
                [xs[k].reshape(far * rows, d.block) for k in places], axis=0
            )
            result = product(0, left, wbuf[0][...].reshape(d.block, d.cols(0)))
            for i, k in enumerate(places):
                for z in range(far):
                    at = (i * far + z) * rows
                    zmine[0][z, k] = result[at : at + rows]
            for step in reversed(range(1, far)):
                z = lax.rem(h + step, far)
                for k in places:
                    src, dst = zmine[0].at[z, k], zin[0].at[h, k]
                    send(src, dst, z_sem.at[0], z * near + l, tp, via=via_z[0])
            return
        result = product(g, xs[...].reshape(n_kv * rows, d.block), weights(g))
        for k in range(near):
            for z in range(far):
                at = (k * far + z) * rows
                zmine[g][z, k] = result[at : at + rows]
        via = meter(zmine[g], far - 1)
        for step in reversed(range(1, far)):
            z = lax.rem(h + step, far)
            send(zmine[g].at[z], zin[g].at[h], z_sem.at[g], z * near + l, tp, via=via)

    early()
    mark('tokp_wait')
    for step in range(1, near):
        k = lax.rem(l + near - step, near)
        arrive(piece(k, tp), xp_sem.at[k, tp])
        for side in range(1, n_tp):
            t = lax.rem(tp + side, n_tp)
            send(piece(k, tp), piece(k, tp), xp_sem.at[k, tp], me, t, via=via_x)
    for step in range(1, near):
        k = lax.rem(l + near - step, near)
        for side in range(1, n_tp):
            t = lax.rem(tp + n_tp - side, n_tp)
            arrive(piece(k, t), xp_sem.at[k, t])

    def collect(g):
        mark(f'z_wait{g}')
        arrive(first(zin[g], far - 1), z_sem.at[g])
        value = zmine[g][h].astype(F32)
        for step in range(1, far):
            z = lax.rem(h + far - step, far)
            value = value + zin[g][z].astype(F32)
        red[g][...] = value.astype(BF16)
        back[g][l] = red[g][l]
        via = meter(red[g], near - 1)
        for step in range(1, near):
            k = lax.rem(l + step, near)
            send(red[g].at[k], back[g].at[l], b_sem.at[g], h * near + k, tp, via=via)

    def rounded(piece):
        return (piece.astype(F32) * scale).astype(BF16).astype(F32)

    via_y = {}

    def advance(g):
        mark(f'b_wait{g}')
        arrive(first(back[g], near - 1), b_sem.at[g])
        cv, cn = span(g, gw), span(g, N)
        mark(f'advance{g}')
        gate = jnp.concatenate([rounded(back[g][k, :, 0:part]) for k in range(near)], axis=1)
        value = jnp.concatenate(
            [rounded(back[g][k, :, part : 2 * part]) for k in range(near)], axis=1
        )

        def unit(u):
            j, k = u // near, u % near
            return rounded(back[j * near // 2][k, :, 2 * part : 2 * part + N])

        def window(past, now, out, cols):
            before = old(past, cols)
            rows_now = []
            for i in range(d.taps - 1):
                row = before[i + 1]
                for a in range(2, props + 1):
                    row = jnp.where(taken == a, before[i + a], row)
                rows_now.append(row)
            rows_now = rows_now + pieces(now)
            for i, row in enumerate(rows_now):
                out[i, :, cols] = row.astype(BF16)
            return rows_now

        win_v = window(past_v, value, next_v, cv)
        win_b = window(past_b, unit(2 * g), next_b, cn)
        win_c = window(past_c, unit(2 * g + 1), next_c, cn)
        x = [silu(v) for v in conv(win_v, taps(conv_v, cv), props)]
        b = [silu(v) for v in conv(win_b, taps(conv_b, cn), props)]
        c = [silu(v) for v in conv(win_c, taps(conv_c, cn), props)]
        whole = jnp.concatenate(c, axis=0)
        masked = jnp.concatenate(
            [jnp.where(row_seq == s, whole, 0.0) for s in range(S)], axis=1
        ).astype(BF16)
        carried = pieces(
            lax.dot_general(masked, rootb[g][...], NT, preferred_element_type=F32)
        )
        dt = pieces(
            softplus(jnp.dot(step_now, spread(g), preferred_element_type=F32) + param(0, g))
        )
        rate = jnp.exp(param(1, g))
        logs = []
        for t in range(props):
            log = -rate * dt[t]
            logs.append(log if t == 0 else logs[-1] + log)
        y = []
        for t in range(props):
            row = jnp.exp(logs[t]) * carried[t] + param(2, g) * x[t]
            for s in range(t + 1):
                score = jnp.sum(c[t] * b[s], axis=-1, keepdims=True)
                weight = dt[s] if s == t else jnp.exp(logs[t] - logs[s]) * dt[s]
                row = row + (score * weight) * x[s]
            y.append(row)
        gated = jnp.concatenate(y, axis=0) * silu(gate)
        mean = jnp.sum(gated * gated, axis=-1, keepdims=True) * (1.0 / gw)
        normal = (gated * lax.rsqrt(mean + EPSILON) * gain_out[:, cv]).astype(BF16)
        if g == last:
            ylast[l] = normal
            via = meter(ylast, near - 1)
            for step in range(1, near):
                k = lax.rem(l + step, near)
                send(ylast.at[l], ylast.at[l], yl_sem.at[0], h * near + k, tp, via=via)
            return
        ys[g][me] = normal
        via_y[g] = meter(ys[g], n_kv - 1)
        for step in reversed(range(1, far)):
            z = lax.rem(h + step, far)
            spot = ys[g].at[me]
            send(spot, spot, yz_sem.at[g], z * near + l, tp, via=via_y[g])
        for step in range(1, near):
            k = lax.rem(l + step, near)
            send(spot, spot, yp_sem.at[g], h * near + k, tp, via=via_y[g])

    def forward(g):
        mark(f'yz_wait{g}')
        arrive(first(ys[g], far - 1), yz_sem.at[g])
        for step in range(1, far):
            spot = ys[g].at[lax.rem(h + far - step, far) * near + l]
            for side in range(1, near):
                k = lax.rem(l + side, near)
                send(spot, spot, yp_sem.at[g], h * near + k, tp, via=via_y[g])

    def output(g):
        mark(f'y_wait{g}')
        arrive(first(ys[g], (near - 1) * far), yp_sem.at[g])
        if g == 0:
            wout_load.wait()
        mark(f'out{g}')
        term = jnp.dot(
            ys[g][...].reshape(n_kv * rows, gw), wout[span(g, gw), :], preferred_element_type=F32
        )
        if g == 0:
            acc[...] = term
        else:
            acc[...] += term

    cols = d.out_cols
    per = n_kv // n_tp
    side, place = lax.div(me, per), lax.rem(me, per)
    deep = per // near

    def share():
        mark('share')
        mine[...] = acc[...].astype(BF16).reshape(n_kv, rows, cols)
        via = meter(mine, n_kv - 1)
        slot = parts.at[tp * per + place]
        for step in range(1, n_kv):
            k = lax.rem(me + step, n_kv)
            send(mine.at[k], slot, m_sem.at[0], k, side, via=via)
        send(mine.at[me], slot, m_sem.at[0], me, side, side != tp)

        @pl.when(side == tp)
        def _():
            parts[tp * per + place] = mine[me]

    def output_last():
        mark('wl_wait')
        for level in levels:
            relay(level)
        if not last:
            wout_load.wait()
        mark('yl_wait')
        arrive(first(ylast, near - 1), yl_sem.at[0])
        mark('outl')
        every = ylast[...].reshape(near * rows, gw)
        for z in range(far):
            term = jnp.dot(every, wlast[z], preferred_element_type=F32).astype(BF16)
            for k in range(near):
                mine_l[z // deep * near + k, z % deep] = term[k * rows : (k + 1) * rows]
        via = meter(mine_l, near * n_tp - 1)
        spot = tp * near + l
        for step in range(1, near * n_tp):
            to = lax.rem(spot + step, near * n_tp)
            send(
                mine_l.at[to], parts_l.at[spot], ml_sem.at[0],
                h * near + lax.rem(to, near), lax.div(to, near), via=via,
            )
        parts_l[spot] = mine_l[spot]

    plan = (
        (project, lambda g: 2.75 * g),
        (collect, lambda g: 8.0 + 3.0 * g if g else 5.6),
        (advance, lambda g: 12.0 + 2.7 * g if g else 9.0),
        (forward, lambda g: 17.2 + 2.1 * g),
    )
    order_of = sorted(
        (when(g), i, g)
        for i, (_, when) in enumerate(plan)
        for g in range(G if i < 3 else last)
    )
    levels = iter(range(1, far))
    for _, i, g in order_of:
        plan[i][0](g)
        if far > 3 and g == last - 1 and i > 1:
            relay(next(levels))

    for g in range(last):
        output(g)
    if last:
        share()
    output_last()

    mark('final_wait')
    if last:
        arrive(first(parts, n_kv - 1), m_sem.at[0], side == tp)
        arrive(parts, m_sem.at[0], side != tp)
    mark('final_last')
    arrive(first(parts_l, near * n_tp - 1), ml_sem.at[0])
    for k in range(per):
        value = None
        for t in range(n_tp):
            terms = [parts_l[t * near + k % near, k // near]]
            terms = terms + ([parts[t * per + k]] if last else [])
            for term in terms:
                term = term.astype(F32)
                value = term if value is None else value + term
        put_seq(mixed, span(k, cols), value.astype(BF16))
    mark('drain')
    for size, at, cond in drains:
        copy = remote(size, size, ssem.at[at], l_sem.at[0], me, tp)
        if cond is None:
            copy.wait_send()
        else:
            pl.when(cond)(copy.wait_send)
    mark(None)


def mixer(d, args):
    G, near, far, rows, n_kv = d.groups, d.near, d.far, d.rows, d.n_kv
    dma = pltpu.SemaphoreType.DMA
    vmem, hbm = pl.BlockSpec(memory_space=pltpu.VMEM), pl.BlockSpec(memory_space=pltpu.HBM)

    def each(shape):
        return [pltpu.VMEM(shape(g), BF16) for g in range(G)]

    scratch = (
        each(lambda g: (near, d.depth, d.cols(g)))
        + each(lambda g: (near, d.depth, d.cols(g)))
        + each(lambda g: (far, near, rows, d.cols(g)))
        + each(lambda g: (far, near, rows, d.cols(g)))
        + each(lambda g: (near, rows, d.cols(g)))
        + each(lambda g: (near, rows, d.cols(g)))
        + each(lambda g: (d.gw, d.seqs * STATE_DIM))
        + each(lambda g: (n_kv, rows, d.gw))[: G - 1]
    )
    nb = d.feats // d.block
    hpad = -(-d.heads // LANES) * LANES
    per = n_kv // d.n_tp
    n_send = nb * d.n_tp + d.n_tp - 1 + 1 + 3 * G + G - 1 + 1 + 2 + 1 + 2 * (far - 1)
    n_local = G + 2 + len(args) - 6
    scratch = scratch + [
        pltpu.VMEM((nb, rows, d.block), BF16),
        pltpu.VMEM((near, far, rows, d.block), BF16),
        pltpu.VMEM((d.n_tp, rows, hpad + LANES), F32),
        pltpu.VMEM((d.n_tp, rows, hpad + LANES), F32),
        pltpu.VMEM((G * d.gw, d.out_cols), BF16),
        pltpu.VMEM((n_kv * rows, d.out_cols), F32),
        pltpu.VMEM((n_kv, rows, d.out_cols), BF16),
        pltpu.VMEM((n_kv, rows, d.out_cols), BF16),
        pltpu.VMEM((far, d.gw, d.out_cols), BF16),
        pltpu.VMEM((near, rows, d.gw), BF16),
        pltpu.VMEM((d.n_tp * near, per // near, rows, d.out_cols), BF16),
        pltpu.VMEM((d.n_tp * near, per // near, rows, d.out_cols), BF16),
        dma((n_send,)), dma((G,)), dma((far,)), dma((near, d.n_tp)), dma((d.n_tp,)),
        dma((G,)), dma((G,)), dma((max(G - 1, 1),)), dma((max(G - 1, 1),)), dma((1,)),
        dma((far,)), dma((1,)), dma((1,)), dma((n_local,)), dma((G,)),
    ]
    scratch = scratch + [pltpu.VMEM(item.shape, item.dtype) for item in args[6:]]
    past_v, past_b, past_c = (item.shape for item in args[-5:-2])
    return pl.pallas_call(
        functools.partial(mixer_kernel, d),
        out_shape=[
            pltpu.VMEM((d.seqs, d.props, d.feats), BF16),
            pltpu.VMEM((d.seqs, G * d.gw, STATE_DIM), F32),
            pltpu.VMEM(past_v, BF16),
            pltpu.VMEM(past_b, BF16),
            pltpu.VMEM(past_c, BF16),
            pltpu.VMEM((d.seqs, d.props, d.heads), BF16),
        ],
        in_specs=[hbm] * len(args),
        out_specs=[vmem] * 6,
        scratch_shapes=scratch,
        compiler_params=pltpu.CompilerParams(
            collective_id=0, has_side_effects=True, vmem_limit_bytes=24 * 2**20
        ),
        name="mixer",
    )(*(pltpu.with_memory_space_constraint(item, pltpu.HBM) for item in args))


def store_kernel(count, *refs):
    sem = refs[-1]
    copies = [
        pltpu.make_async_copy(refs[i], refs[count + i], sem.at[i]) for i in range(count)
    ]
    for copy in copies:
        copy.start()
    for copy in copies:
        copy.wait()


def store(items):
    count = len(items)
    return pl.pallas_call(
        functools.partial(store_kernel, count),
        out_shape=[jax.ShapeDtypeStruct(item.shape, item.dtype) for item in items],
        in_specs=[pl.BlockSpec(memory_space=pltpu.VMEM)] * count,
        out_specs=[pl.BlockSpec(memory_space=pltpu.HBM)] * count,
        scratch_shapes=[pltpu.SemaphoreType.DMA((count,))],
        compiler_params=pltpu.CompilerParams(vmem_limit_bytes=2**20),
        name="store",
    )(*items)


def on_device(
    tokens, input_gain, gate_weight, value_weight, write_weight, read_weight, step_weight,
    conv_value, conv_write, conv_read, step_bias, decay_log, skip_gain, output_gain, out_weight,
    base_state, past_value, past_write, past_read, past_step, accepted,
):
    seqs, props, feats = tokens.shape
    n_kv, n_tp = lax.axis_size("kv"), lax.axis_size("tp")
    depth, inner = gate_weight.shape
    groups = write_weight.shape[1] // STATE_DIM
    heads = step_bias.shape[0]
    gw = inner // groups
    near = near_size(n_kv, gw)
    d = Dims(
        far=n_kv // near, near=near, n_tp=n_tp, seqs=seqs, props=props,
        taps=conv_value.shape[0], width=feats * n_tp, feats=feats, depth=depth, groups=groups,
        gw=gw, heads=heads, out_cols=out_weight.shape[1],
    )

    def major(item):
        return item.transpose(1, 0, 2)

    def line(item):
        return item.reshape(1, item.shape[0])

    outs = mixer(
        d,
        (
            gate_weight, value_weight, write_weight, read_weight, out_weight,
            base_state.reshape(seqs, inner, STATE_DIM),
            tokens, line(input_gain), step_weight.T, conv_value, conv_write, conv_read,
            line(step_bias), line(decay_log), line(skip_gain), line(output_gain),
            major(past_value), major(past_write), major(past_read), past_step, line(accepted),
        ),
    )
    mixed, root, next_v, next_b, next_c, next_s = store(outs)
    return (
        mixed, root.reshape(base_state.shape), major(next_v), major(next_b), major(next_c), next_s,
    )


def solution(mesh):
    split = P("kv", None, "tp")
    weight = P("kv", "tp")
    state = P("kv", "tp", None, None)
    return jax.shard_map(
        on_device,
        mesh=mesh,
        in_specs=(
            split, P(), weight, weight, weight, weight, P(),
            P(None, "tp"), P(None, "tp"), P(None, "tp"),
            P("tp"), P("tp"), P("tp"), P("tp"),
            P("tp", "kv"),
            state, split, split, split, split, P("kv"),
        ),
        out_specs=(split, state, split, split, split, split),
        check_vma=False,
    )
```

```python
import functools
from typing import NamedTuple

import jax
import jax.numpy as jnp
from jax import lax
from jax.experimental import pallas as pl
from jax.experimental.pallas import tpu as pltpu
from jax.sharding import PartitionSpec as P

STATE_DIM = 128
LANES = 128
SMALL = 21
EPSILON = 1e-06
MESH = pl.DeviceIdType.MESH
F32 = jnp.float32
BF16 = jnp.bfloat16


class Dims(NamedTuple):
    far: int
    near: int
    n_tp: int
    seqs: int
    props: int
    taps: int
    width: int
    feats: int
    depth: int
    groups: int
    gw: int
    heads: int
    out_cols: int

    @property
    def rows(self):
        return self.seqs * self.props

    @property
    def n_kv(self):
        return self.far * self.near

    @property
    def block(self):
        return self.near * self.depth

    @property
    def part(self):
        return self.gw // self.near

    def thin(self, g):
        return 2 * g % self.near == 0

    def cols(self, g):
        return 2 * self.part + (STATE_DIM if self.thin(g) else 0)


def near_size(n_kv, gw):
    return max(
        d
        for d in range(2, n_kv + 1, 2)
        if n_kv % d == 0 and d * d <= n_kv and gw % (LANES * d) == 0
    )


def remote(src, dst, send, recv, kv, tp):
    return pltpu.make_async_remote_copy(
        src_ref=src,
        dst_ref=dst,
        send_sem=send,
        recv_sem=recv,
        device_id={"kv": kv, "tp": tp},
        device_id_type=MESH,
    )


def silu(v):
    return v / (1.0 + jnp.exp(-v))


def softplus(v):
    return jnp.maximum(v, 0.0) + jnp.log1p(jnp.exp(-jnp.abs(v)))


def conv(rows, taps, count):
    out = []
    for t in range(count):
        total = taps[0] * rows[t]
        for k in range(1, len(taps)):
            total = total + taps[k] * rows[t + k]
        out.append(total)
    return out


NT = (((1,), (1,)), ((), ()))


def mixer_kernel(d, *refs):
    gate_w, value_w, write_w, read_w, wout_h, base_h = refs[:6]
    small = refs[6:SMALL]
    mixed, base_v, next_v, next_b, next_c, next_s = refs[SMALL : SMALL + 6]
    rest = list(refs[SMALL + 6 :])
    G = d.groups
    stage, wbuf, zmine, zin, red, back, rootb = (rest[i * G : (i + 1) * G] for i in range(7))
    ys, rest = rest[7 * G : 8 * G - 1], rest[8 * G - 1 :]
    last = G - 1
    (
        xq, xs, pt_mine, pt_in, wout, acc, mine, parts, wlast, ylast, mine_l, parts_l,
        ssem, w_sem, xz_sem, xp_sem, pt_sem, z_sem, b_sem, yz_sem, yp_sem, m_sem,
        wl_sem, yl_sem, ml_sem, l_sem, g_sem,
    ) = rest[:27]
    held = rest[27:]
    (
        tok, gain, step_w, conv_v, conv_b, conv_c, bias_r, decay_r, skip_r, gain_out,
        past_v, past_b, past_c, past_s, taken_ref,
    ) = held
    far, near, n_tp, rows, S, N = d.far, d.near, d.n_tp, d.rows, d.seqs, STATE_DIM
    n_kv, part, gw, props = d.n_kv, d.part, d.gw, d.props
    me, tp = lax.axis_index("kv"), lax.axis_index("tp")
    h, l = lax.div(me, near), lax.rem(me, near)

    barrier = pltpu.get_barrier_semaphore()

    def greet(kv, t):
        pl.semaphore_signal(barrier, inc=1, device_id={"kv": kv, "tp": t}, device_id_type=MESH)

    for step in range(1, near):
        greet(h * near + lax.rem(l + step, near), tp)
    for t in range(n_tp):
        for step in range(1, far):
            greet(lax.rem(h + step, far) * near + l, t)
    for step in range(1, n_tp):
        greet(me, lax.rem(tp + step, n_tp))
    greeted = near - 1 + (far - 1) * n_tp + n_tp - 1

    class Mark:
        scope = None

        def __call__(self, name):
            if self.scope is not None:
                self.scope.__exit__(None, None, None)
            self.scope = None
            if name is not None:
                self.scope = jax.named_scope(name)
                self.scope.__enter__()

    mark = Mark()
    mark("prologue")
    used = []

    def local(src, dst):
        copy = pltpu.make_async_copy(src, dst, l_sem.at[len(used)])
        copy.start()
        used.append(copy)
        return copy

    fetch = [local(src, dst) for src, dst in zip(small, held)]
    units = 2 * G
    for g in range(G):
        def stage_in(src, dst):
            pltpu.make_async_copy(src, dst, g_sem.at[g]).start()

        for k in range(near):
            lo = g * gw + k * part
            stage_in(gate_w.at[:, lo : lo + part], stage[g].at[k, :, 0:part])
            stage_in(value_w.at[:, lo : lo + part], stage[g].at[k, :, part : 2 * part])
            if d.thin(g):
                u = (2 * g + k) % units
                source = (write_w, read_w)[u % 2]
                stage_in(
                    source.at[:, u // 2 * N : (u // 2 + 1) * N],
                    stage[g].at[k, :, 2 * part : 2 * part + N],
                )
    loading = [
        local(base_h.at[:, g * gw : (g + 1) * gw], base_v.at[:, g * gw : (g + 1) * gw])
        for g in range(G)
    ]
    wlast_load = local(wout_h.at[last * gw : G * gw], wlast.at[h])
    wout_load = local(wout_h, wout)

    drains = []

    def meter(ref, count):
        at = len(drains)
        size = ref if count is None else ref.at[pl.ds(0, count)]
        drains.append((size, at, None))
        return at

    def alone(src, cond=None):
        drains.append((src, len(drains), cond))
        return len(drains) - 1

    def send(src, dst, recv, kv, t, cond=None, via=None):
        at = alone(src, cond) if via is None else via
        copy = remote(src, dst, ssem.at[at], recv, kv, t)
        if cond is None:
            copy.start()
        else:
            pl.when(cond)(copy.start)

    def arrive(dst, recv, cond=None):
        copy = remote(dst, dst, ssem.at[0], recv, me, tp)
        if cond is None:
            copy.wait_recv()
        else:
            pl.when(cond)(copy.wait_recv)

    def first(ref, count):
        return ref.at[pl.ds(0, count)]

    nb = d.feats // d.block
    own = pl.multiple_of(tp * d.feats, d.feats)
    for copy in fetch:
        copy.wait()
    order = lax.broadcasted_iota(jnp.int32, (rows, rows), 0)
    other = lax.broadcasted_iota(jnp.int32, (rows, rows), 1)

    def shuffle(major, minor):
        source = lax.rem(order, minor) * major + lax.div(order, minor)
        return jnp.where(other == source, 1.0, 0.0).astype(BF16)

    to_time, to_seq = shuffle(props, S), shuffle(S, props)

    def time_major(ref):
        stacked = jnp.concatenate([ref[s].astype(F32) for s in range(S)], axis=0).astype(BF16)
        return jnp.dot(to_time, stacked, preferred_element_type=F32)

    def put_seq(ref, cols, value):
        value = jnp.dot(to_seq, value, preferred_element_type=F32)
        for s in range(S):
            ref[s, :, cols] = value[s * props : (s + 1) * props].astype(BF16)

    raw = time_major(tok)
    square = jnp.sum(raw * raw, axis=-1, keepdims=True)
    scaled = (raw * gain[:, pl.ds(own, d.feats)]).astype(BF16)
    for q in range(nb):
        xq[q] = scaled[:, q * d.block : (q + 1) * d.block]
    hpad = pt_mine.shape[2] - LANES
    for t in range(n_tp):
        term = lax.dot_general(
            scaled, step_w[t * d.heads : (t + 1) * d.heads, pl.ds(own, d.feats)], NT,
            preferred_element_type=F32,
        )
        pt_mine[t, :, 0 : d.heads] = term
        pt_mine[t, :, hpad : hpad + LANES] = jnp.broadcast_to(square, (rows, LANES))
    pt_in[tp] = pt_mine[tp]

    mark('barrier')
    pl.semaphore_wait(barrier, greeted)

    mark('tok_send')
    home = lax.div(h, nb)
    for q in range(nb):
        plane = tp * nb + q
        for t in range(n_tp):
            away = jnp.logical_or(plane != h, tp != t)
            send(xq.at[q], xs.at[l, h], xz_sem.at[h], plane * near + l, t, away)

    @pl.when(home == tp)
    def _():
        xs[l, h] = xq[lax.rem(h, nb)]

    for step in range(1, n_tp):
        t = lax.rem(tp + step, n_tp)
        send(pt_mine.at[t], pt_in.at[tp], pt_sem.at[tp], me, t)

    def send_weights(g):
        arrive(stage[g], g_sem.at[g])
        via = meter(stage[g], near - 1)
        for step in range(1, near):
            k = lax.rem(l + step, near)
            send(stage[g].at[k], wbuf[g].at[l], w_sem.at[g], h * near + k, tp, via=via)

    send_weights(0)
    wlast_load.wait()

    def inside(z):
        return jnp.logical_and(z >= 0, z < far)

    def relay(level):
        for way in (1, -1):
            z = h - way * level
            block = lax.rem(z + far, far)
            if level:
                arrive(wlast.at[block], wl_sem.at[block], inside(z))
            if level < far - 1:
                peer = lax.rem(h + way + far, far) * near + l
                go = jnp.logical_and(inside(z), inside(h + way))
                send(wlast.at[block], wlast.at[block], wl_sem.at[block], peer, tp, go)

    diagonal = lax.broadcasted_iota(jnp.int32, (S, S), 0) == lax.broadcasted_iota(
        jnp.int32, (S, S), 1
    )
    taken = jnp.sum(
        jnp.where(diagonal, taken_ref[...].astype(F32), 0.0), axis=-1, keepdims=True
    ).astype(jnp.int32)
    steps_old = time_major(past_s).astype(BF16)
    head_rows = jnp.concatenate(
        [bias_r[...], decay_r[...], skip_r[...]] + [jnp.zeros_like(bias_r[...])] * 5, axis=0
    )
    params = []
    row_seq = lax.rem(lax.broadcasted_iota(jnp.int32, (rows, N), 0), S)

    def spread(g):
        r = lax.broadcasted_iota(jnp.int32, (d.heads, gw), 0)
        c = lax.broadcasted_iota(jnp.int32, (d.heads, gw), 1)
        hw = gw * G // d.heads
        lo = r * hw - g * gw
        return jnp.where(jnp.logical_and(c >= lo, c < lo + hw), 1.0, 0.0).astype(BF16)

    def span(g, w):
        return slice(g * w, (g + 1) * w)

    def taps(ref, cols):
        return [ref[k : k + 1, cols] for k in range(d.taps)]

    def param(k, g):
        if g == len(params):
            params.append(
                jnp.dot(
                    head_rows, spread(g).astype(F32), preferred_element_type=F32,
                    precision=lax.Precision.HIGHEST,
                )
            )
        return params[g][k : k + 1]

    def pieces(v):
        return [v[t * S : (t + 1) * S] for t in range(props)]

    def old(ref, cols):
        return [ref[i, :, cols].astype(F32) for i in range(ref.shape[0])]

    def root(g):
        mark(f'root{g}')
        loading[g].wait()
        cv, cn = span(g, gw), span(g, N)
        px = [silu(v) for v in conv(old(past_v, cv), taps(conv_v, cv), props)]
        pb = [silu(v) for v in conv(old(past_b, cn), taps(conv_b, cn), props)]
        pd = softplus(
            jnp.dot(steps_old, spread(g), preferred_element_type=F32) + param(0, g)
        )
        rate = jnp.exp(param(1, g))
        pd = pieces(pd)
        log = [jnp.where(taken > t, -rate * pd[t], 0.0) for t in range(props)]
        tail = jnp.zeros_like(log[0])
        weighted = [None] * props
        for t in reversed(range(props)):
            weighted[t] = jnp.where(taken > t, jnp.exp(tail) * pd[t], 0.0) * px[t]
            tail = tail + log[t]
        left = jnp.transpose(jnp.concatenate(weighted, axis=0)).astype(BF16)
        decay = jnp.exp(tail)
        fill = [decay] * max(1, 8 // S)
        decay = jnp.transpose(jnp.concatenate(fill, axis=0))
        right = jnp.concatenate(pb, axis=0)
        for s in range(S):
            outer = jnp.dot(
                left,
                jnp.where(row_seq == s, right, 0.0).astype(BF16),
                preferred_element_type=F32,
            )
            new = decay[:, s : s + 1] * base_v[s, cv, :] + outer
            base_v[s, cv, :] = new
            rootb[g][:, span(s, N)] = new.astype(BF16)

    for g in range(max(1, G - 1)):
        root(g)

    mark('tokz_wait')
    for k in range(far):
        arrive(
            xs.at[l, k], xz_sem.at[k], jnp.logical_or(h != k, home != tp)
        )
    fq = far // n_tp

    def piece(k, t):
        return xs.at[k, pl.ds(t * fq, fq)]

    via_x = meter(xs, near - 1)
    for step in range(1, near):
        k = h * near + lax.rem(l + step, near)
        send(piece(l, tp), piece(l, tp), xp_sem.at[l, tp], k, tp, via=via_x)
    for g in range(1, G):
        send_weights(g)
    relay(0)
    if G > 1:
        root(G - 1)

    mark('scale')
    for step in range(1, n_tp):
        t = lax.rem(tp + n_tp - step, n_tp)
        arrive(pt_in.at[t], pt_sem.at[t])
    joined = pt_in[0]
    for t in range(1, n_tp):
        joined = joined + pt_in[t]
    scale = lax.rsqrt(joined[:, hpad : hpad + LANES] * (1.0 / d.width) + EPSILON)
    step_now = (joined[:, 0 : d.heads] * scale[:, 0 : d.heads]).astype(BF16)
    put_seq(next_s, slice(None), step_now)

    def weights(g):
        mark(f'w_wait{g}')
        wbuf[g][l] = stage[g][l]
        arrive(first(wbuf[g], near - 1), w_sem.at[g])
        mark(f'matmul{g}')
        return wbuf[g][...].reshape(d.block, d.cols(g))

    def product(g, left, weight):
        return jnp.dot(left, weight, preferred_element_type=F32).astype(BF16)

    via_z = {}

    def early():
        result = product(0, xs[l].reshape(far * rows, d.block), weights(0))
        for z in range(far):
            zmine[0][z, l] = result[z * rows : (z + 1) * rows]
        via_z[0] = meter(zmine[0], far - 1)
        for step in reversed(range(1, far)):
            z = lax.rem(h + step, far)
            src, dst = zmine[0].at[z, l], zin[0].at[h, l]
            send(src, dst, z_sem.at[0], z * near + l, tp, via=via_z[0])

    def batch(t):
        places = [lax.rem(l + step, near) for step in range(1, near)]
        left = jnp.concatenate(
            [xs[k, pl.ds(t * fq, fq)].reshape(fq * rows, d.block) for k in places], axis=0
        )
        result = product(0, left, wbuf[0][...].reshape(d.block, d.cols(0)))
        for i, k in enumerate(places):
            for q in range(fq):
                at = (i * fq + q) * rows
                zmine[0][t * fq + q, k] = result[at : at + rows]
        for q in range(fq):
            z = t * fq + q
            for k in places:
                src, dst = zmine[0].at[z, k], zin[0].at[h, k]
                send(src, dst, z_sem.at[0], z * near + l, tp, z != h, via=via_z[0])

    def project(g):
        if g == 0:
            for side in range(1, n_tp):
                batch(lax.rem(tp + side, n_tp))
            return
        result = product(g, xs[...].reshape(n_kv * rows, d.block), weights(g))
        for k in range(near):
            for z in range(far):
                at = (k * far + z) * rows
                zmine[g][z, k] = result[at : at + rows]
        via = meter(zmine[g], far - 1)
        for step in reversed(range(1, far)):
            z = lax.rem(h + step, far)
            send(zmine[g].at[z], zin[g].at[h], z_sem.at[g], z * near + l, tp, via=via)

    early()
    mark('tokp_wait')
    for step in range(1, near):
        k = lax.rem(l + near - step, near)
        arrive(piece(k, tp), xp_sem.at[k, tp])
        for side in range(1, n_tp):
            t = lax.rem(tp + side, n_tp)
            send(piece(k, tp), piece(k, tp), xp_sem.at[k, tp], me, t, via=via_x)
    batch(tp)
    for step in range(1, near):
        k = lax.rem(l + near - step, near)
        for side in range(1, n_tp):
            t = lax.rem(tp + n_tp - side, n_tp)
            arrive(piece(k, t), xp_sem.at[k, t])

    def collect(g):
        mark(f'z_wait{g}')
        arrive(first(zin[g], far - 1), z_sem.at[g])
        value = zmine[g][h].astype(F32)
        for step in range(1, far):
            z = lax.rem(h + far - step, far)
            value = value + zin[g][z].astype(F32)
        red[g][...] = value.astype(BF16)
        back[g][l] = red[g][l]
        via = meter(red[g], near - 1)
        for step in range(1, near):
            k = lax.rem(l + step, near)
            send(red[g].at[k], back[g].at[l], b_sem.at[g], h * near + k, tp, via=via)

    def rounded(piece):
        return (piece.astype(F32) * scale).astype(BF16).astype(F32)

    via_y = {}

    def advance(g):
        mark(f'b_wait{g}')
        arrive(first(back[g], near - 1), b_sem.at[g])
        cv, cn = span(g, gw), span(g, N)
        mark(f'advance{g}')
        gate = jnp.concatenate([rounded(back[g][k, :, 0:part]) for k in range(near)], axis=1)
        value = jnp.concatenate(
            [rounded(back[g][k, :, part : 2 * part]) for k in range(near)], axis=1
        )

        def unit(u):
            j, k = u // near, u % near
            return rounded(back[j * near // 2][k, :, 2 * part : 2 * part + N])

        def window(past, now, out, cols):
            before = old(past, cols)
            rows_now = []
            for i in range(d.taps - 1):
                row = before[i + 1]
                for a in range(2, props + 1):
                    row = jnp.where(taken == a, before[i + a], row)
                rows_now.append(row)
            rows_now = rows_now + pieces(now)
            for i, row in enumerate(rows_now):
                out[i, :, cols] = row.astype(BF16)
            return rows_now

        win_v = window(past_v, value, next_v, cv)
        win_b = window(past_b, unit(2 * g), next_b, cn)
        win_c = window(past_c, unit(2 * g + 1), next_c, cn)
        x = [silu(v) for v in conv(win_v, taps(conv_v, cv), props)]
        b = [silu(v) for v in conv(win_b, taps(conv_b, cn), props)]
        c = [silu(v) for v in conv(win_c, taps(conv_c, cn), props)]
        whole = jnp.concatenate(c, axis=0)
        masked = jnp.concatenate(
            [jnp.where(row_seq == s, whole, 0.0) for s in range(S)], axis=1
        ).astype(BF16)
        carried = pieces(
            lax.dot_general(masked, rootb[g][...], NT, preferred_element_type=F32)
        )
        dt = pieces(
            softplus(jnp.dot(step_now, spread(g), preferred_element_type=F32) + param(0, g))
        )
        rate = jnp.exp(param(1, g))
        logs = []
        for t in range(props):
            log = -rate * dt[t]
            logs.append(log if t == 0 else logs[-1] + log)
        y = []
        for t in range(props):
            row = jnp.exp(logs[t]) * carried[t] + param(2, g) * x[t]
            for s in range(t + 1):
                score = jnp.sum(c[t] * b[s], axis=-1, keepdims=True)
                weight = dt[s] if s == t else jnp.exp(logs[t] - logs[s]) * dt[s]
                row = row + (score * weight) * x[s]
            y.append(row)
        gated = jnp.concatenate(y, axis=0) * silu(gate)
        mean = jnp.sum(gated * gated, axis=-1, keepdims=True) * (1.0 / gw)
        normal = (gated * lax.rsqrt(mean + EPSILON) * gain_out[:, cv]).astype(BF16)
        if g == last:
            ylast[l] = normal
            via = meter(ylast, near - 1)
            for step in range(1, near):
                k = lax.rem(l + step, near)
                send(ylast.at[l], ylast.at[l], yl_sem.at[0], h * near + k, tp, via=via)
            return
        ys[g][me] = normal
        via_y[g] = meter(ys[g], n_kv - 1)
        for step in reversed(range(1, far)):
            z = lax.rem(h + step, far)
            spot = ys[g].at[me]
            send(spot, spot, yz_sem.at[g], z * near + l, tp, via=via_y[g])
        for step in range(1, near):
            k = lax.rem(l + step, near)
            send(spot, spot, yp_sem.at[g], h * near + k, tp, via=via_y[g])

    def forward(g):
        mark(f'yz_wait{g}')
        arrive(first(ys[g], far - 1), yz_sem.at[g])
        for step in range(1, far):
            spot = ys[g].at[lax.rem(h + far - step, far) * near + l]
            for side in range(1, near):
                k = lax.rem(l + side, near)
                send(spot, spot, yp_sem.at[g], h * near + k, tp, via=via_y[g])

    def output(g):
        mark(f'y_wait{g}')
        arrive(first(ys[g], (near - 1) * far), yp_sem.at[g])
        if g == 0:
            wout_load.wait()
        mark(f'out{g}')
        term = jnp.dot(
            ys[g][...].reshape(n_kv * rows, gw), wout[span(g, gw), :], preferred_element_type=F32
        )
        if g == 0:
            acc[...] = term
        else:
            acc[...] += term

    cols = d.out_cols
    per = n_kv // n_tp
    side, place = lax.div(me, per), lax.rem(me, per)
    deep = per // near

    def share():
        mark('share')
        mine[...] = acc[...].astype(BF16).reshape(n_kv, rows, cols)
        via = meter(mine, n_kv - 1)
        slot = parts.at[tp * per + place]
        for step in range(1, n_kv):
            k = lax.rem(me + step, n_kv)
            send(mine.at[k], slot, m_sem.at[0], k, side, via=via)
        send(mine.at[me], slot, m_sem.at[0], me, side, side != tp)

        @pl.when(side == tp)
        def _():
            parts[tp * per + place] = mine[me]

    def output_last():
        mark('wl_wait')
        for level in levels:
            relay(level)
        if not last:
            wout_load.wait()
        mark('yl_wait')
        arrive(first(ylast, near - 1), yl_sem.at[0])
        mark('outl')
        every = ylast[...].reshape(near * rows, gw)
        for z in range(far):
            term = jnp.dot(every, wlast[z], preferred_element_type=F32).astype(BF16)
            for k in range(near):
                mine_l[z // deep * near + k, z % deep] = term[k * rows : (k + 1) * rows]
        via = meter(mine_l, near * n_tp - 1)
        spot = tp * near + l
        for step in range(1, near * n_tp):
            to = lax.rem(spot + step, near * n_tp)
            send(
                mine_l.at[to], parts_l.at[spot], ml_sem.at[0],
                h * near + lax.rem(to, near), lax.div(to, near), via=via,
            )
        parts_l[spot] = mine_l[spot]

    plan = (
        (project, lambda g: 2.75 * g),
        (collect, lambda g: 8.0 + 3.0 * g if g else 5.6),
        (advance, lambda g: 12.0 + 2.7 * g if g else 9.0),
        (forward, lambda g: 17.2 + 2.1 * g),
    )
    order_of = sorted(
        (when(g), i, g)
        for i, (_, when) in enumerate(plan)
        for g in range(G if i < 3 else last)
    )
    levels = iter(range(1, far))
    for _, i, g in order_of:
        plan[i][0](g)
        if far > 3 and g == last - 1 and i > 1:
            relay(next(levels))

    for g in range(last):
        output(g)
    if last:
        share()
    output_last()

    mark('final_wait')
    if last:
        arrive(first(parts, n_kv - 1), m_sem.at[0], side == tp)
        arrive(parts, m_sem.at[0], side != tp)
    mark('final_last')
    arrive(first(parts_l, near * n_tp - 1), ml_sem.at[0])
    for k in range(per):
        value = None
        for t in range(n_tp):
            terms = [parts_l[t * near + k % near, k // near]]
            terms = terms + ([parts[t * per + k]] if last else [])
            for term in terms:
                term = term.astype(F32)
                value = term if value is None else value + term
        put_seq(mixed, span(k, cols), value.astype(BF16))
    mark('drain')
    for size, at, cond in drains:
        copy = remote(size, size, ssem.at[at], l_sem.at[0], me, tp)
        if cond is None:
            copy.wait_send()
        else:
            pl.when(cond)(copy.wait_send)
    mark(None)


def mixer(d, args):
    G, near, far, rows, n_kv = d.groups, d.near, d.far, d.rows, d.n_kv
    dma = pltpu.SemaphoreType.DMA
    vmem, hbm = pl.BlockSpec(memory_space=pltpu.VMEM), pl.BlockSpec(memory_space=pltpu.HBM)

    def each(shape):
        return [pltpu.VMEM(shape(g), BF16) for g in range(G)]

    scratch = (
        each(lambda g: (near, d.depth, d.cols(g)))
        + each(lambda g: (near, d.depth, d.cols(g)))
        + each(lambda g: (far, near, rows, d.cols(g)))
        + each(lambda g: (far, near, rows, d.cols(g)))
        + each(lambda g: (near, rows, d.cols(g)))
        + each(lambda g: (near, rows, d.cols(g)))
        + each(lambda g: (d.gw, d.seqs * STATE_DIM))
        + each(lambda g: (n_kv, rows, d.gw))[: G - 1]
    )
    nb = d.feats // d.block
    hpad = -(-d.heads // LANES) * LANES
    per = n_kv // d.n_tp
    n_send = nb * d.n_tp + d.n_tp - 1 + 1 + 3 * G + G - 1 + 1 + 2 + 1 + 2 * (far - 1)
    n_local = G + 2 + len(args) - 6
    scratch = scratch + [
        pltpu.VMEM((nb, rows, d.block), BF16),
        pltpu.VMEM((near, far, rows, d.block), BF16),
        pltpu.VMEM((d.n_tp, rows, hpad + LANES), F32),
        pltpu.VMEM((d.n_tp, rows, hpad + LANES), F32),
        pltpu.VMEM((G * d.gw, d.out_cols), BF16),
        pltpu.VMEM((n_kv * rows, d.out_cols), F32),
        pltpu.VMEM((n_kv, rows, d.out_cols), BF16),
        pltpu.VMEM((n_kv, rows, d.out_cols), BF16),
        pltpu.VMEM((far, d.gw, d.out_cols), BF16),
        pltpu.VMEM((near, rows, d.gw), BF16),
        pltpu.VMEM((d.n_tp * near, per // near, rows, d.out_cols), BF16),
        pltpu.VMEM((d.n_tp * near, per // near, rows, d.out_cols), BF16),
        dma((n_send,)), dma((G,)), dma((far,)), dma((near, d.n_tp)), dma((d.n_tp,)),
        dma((G,)), dma((G,)), dma((max(G - 1, 1),)), dma((max(G - 1, 1),)), dma((1,)),
        dma((far,)), dma((1,)), dma((1,)), dma((n_local,)), dma((G,)),
    ]
    scratch = scratch + [pltpu.VMEM(item.shape, item.dtype) for item in args[6:]]
    past_v, past_b, past_c = (item.shape for item in args[-5:-2])
    return pl.pallas_call(
        functools.partial(mixer_kernel, d),
        out_shape=[
            pltpu.VMEM((d.seqs, d.props, d.feats), BF16),
            pltpu.VMEM((d.seqs, G * d.gw, STATE_DIM), F32),
            pltpu.VMEM(past_v, BF16),
            pltpu.VMEM(past_b, BF16),
            pltpu.VMEM(past_c, BF16),
            pltpu.VMEM((d.seqs, d.props, d.heads), BF16),
        ],
        in_specs=[hbm] * len(args),
        out_specs=[vmem] * 6,
        scratch_shapes=scratch,
        compiler_params=pltpu.CompilerParams(
            collective_id=0, has_side_effects=True, vmem_limit_bytes=24 * 2**20
        ),
        name="mixer",
    )(*(pltpu.with_memory_space_constraint(item, pltpu.HBM) for item in args))


def store_kernel(count, *refs):
    sem = refs[-1]
    copies = [
        pltpu.make_async_copy(refs[i], refs[count + i], sem.at[i]) for i in range(count)
    ]
    for copy in copies:
        copy.start()
    for copy in copies:
        copy.wait()


def store(items):
    count = len(items)
    return pl.pallas_call(
        functools.partial(store_kernel, count),
        out_shape=[jax.ShapeDtypeStruct(item.shape, item.dtype) for item in items],
        in_specs=[pl.BlockSpec(memory_space=pltpu.VMEM)] * count,
        out_specs=[pl.BlockSpec(memory_space=pltpu.HBM)] * count,
        scratch_shapes=[pltpu.SemaphoreType.DMA((count,))],
        compiler_params=pltpu.CompilerParams(vmem_limit_bytes=2**20),
        name="store",
    )(*items)


def on_device(
    tokens, input_gain, gate_weight, value_weight, write_weight, read_weight, step_weight,
    conv_value, conv_write, conv_read, step_bias, decay_log, skip_gain, output_gain, out_weight,
    base_state, past_value, past_write, past_read, past_step, accepted,
):
    seqs, props, feats = tokens.shape
    n_kv, n_tp = lax.axis_size("kv"), lax.axis_size("tp")
    depth, inner = gate_weight.shape
    groups = write_weight.shape[1] // STATE_DIM
    heads = step_bias.shape[0]
    gw = inner // groups
    near = near_size(n_kv, gw)
    d = Dims(
        far=n_kv // near, near=near, n_tp=n_tp, seqs=seqs, props=props,
        taps=conv_value.shape[0], width=feats * n_tp, feats=feats, depth=depth, groups=groups,
        gw=gw, heads=heads, out_cols=out_weight.shape[1],
    )

    def major(item):
        return item.transpose(1, 0, 2)

    def line(item):
        return item.reshape(1, item.shape[0])

    outs = mixer(
        d,
        (
            gate_weight, value_weight, write_weight, read_weight, out_weight,
            base_state.reshape(seqs, inner, STATE_DIM),
            tokens, line(input_gain), step_weight.T, conv_value, conv_write, conv_read,
            line(step_bias), line(decay_log), line(skip_gain), line(output_gain),
            major(past_value), major(past_write), major(past_read), past_step, line(accepted),
        ),
    )
    mixed, root, next_v, next_b, next_c, next_s = store(outs)
    return (
        mixed, root.reshape(base_state.shape), major(next_v), major(next_b), major(next_c), next_s,
    )


def solution(mesh):
    split = P("kv", None, "tp")
    weight = P("kv", "tp")
    state = P("kv", "tp", None, None)
    return jax.shard_map(
        on_device,
        mesh=mesh,
        in_specs=(
            split, P(), weight, weight, weight, weight, P(),
            P(None, "tp"), P(None, "tp"), P(None, "tp"),
            P("tp"), P("tp"), P("tp"), P("tp"),
            P("tp", "kv"),
            state, split, split, split, split, P("kv"),
        ),
        out_specs=(split, state, split, split, split, split),
        check_vma=False,
    )
```
